512 devices in a mesh: sp: 32 (over z, x), tp: 16 (over y, core).
Axes of the slice: x: 4, y: 8, z: 8, core: 2. Of those that a mesh axis runs over, the one named last changes fastest.
Arguments:
- query_one: bfloat16 [8192, 1024], P('sp', 'tp'), may hold values from -6 to 6
- key_one: bfloat16 [8192, 1024], P('sp', 'tp'), may hold values from -6 to 6
- value_one: bfloat16 [8192, 2048], P('sp', 'tp'), may hold values from -6 to 6
- gate_one: bfloat16 [8192, 2048], P('sp', 'tp'), may hold values from -6 to 6
- decay_one: float32 [2, 8192, 1024], P(None, 'sp', 'tp')
- query_two: bfloat16 [8192, 2048], P('sp', 'tp'), may hold values from -6 to 6
- key_two: bfloat16 [8192, 2048], P('sp', 'tp'), may hold values from -6 to 6
- value_two: bfloat16 [8192, 2048], P('sp', 'tp'), may hold values from -6 to 6
- gate_two: bfloat16 [8192, 2048], P('sp', 'tp'), may hold values from -6 to 6
- decay_two: float32 [2, 8192, 2048], P(None, 'sp', 'tp')
- head_gain: float32 [128], replicated, may hold values from 0.1 to 1.9
- proj_one: bfloat16 [2048, 2048], P('tp'), may hold values from -0.09375 to 0.09375
- proj_two: bfloat16 [2048, 2048], P('tp'), may hold values from -0.09375 to 0.09375
- stream: bfloat16 [8192, 2048], P('sp'), may hold values from -6 to 6
- gain_mix: float32 [2048], replicated, may hold values from 0.1 to 1.9
- gain_moe: float32 [2048], replicated, may hold values from 0.1 to 1.9
- routes: int32 [8192, 2], P('sp'), may hold values from 0 to 31, all different within a row; in each aligned block of 256 rows (0 to 255, 256 to 511, ...) at most 24 rows name the same one
- affinity: float32 [8192, 2], P('sp'), may hold values from 0.1 to 1
- expert_gate: bfloat16 [32, 2048, 2048], P('sp', None, 'tp'), may hold values from -0.125 to 0.125
- expert_up: bfloat16 [32, 2048, 2048], P('sp', None, 'tp'), may hold values from -0.125 to 0.125
- expert_down: bfloat16 [32, 2048, 2048], P('sp', 'tp'), may hold values from -0.125 to 0.125
Outputs:
- output: bfloat16 [8192, 2048], P(('sp', 'tp'))
The draws below stay inside these ranges and needn't reach their ends.
Inputs may be any that keep to these rules, and one draw needn't show every extreme that they name: `routes`: in the 256 rows of one index of sp no expert is named more than 24 times, a bound that some block reaches there in every draw; a row names 2 different experts.
All inputs are finite; a program needn't handle non-finite values.
Results may differ from the reference program's by a relative error of at most 0.017.
Values may be sent and summed in bfloat16 or wider, within the bound.
No kernel may reach another device: no remote copies, remote signals or barrier semaphores. Data moves between devices by JAX's collectives and lax.ppermute only.
A program may use at most 64 MiB of HBM per device.

```python
import math
import jax
import jax.numpy as jnp
import numpy as np
from jax import lax

D = 2048
HEADS_A = 16
HEADS_B = 16
DK_A = 64
DK_B = 128
DV = 128
BLK = 64
FF_E = 2048
TOPK = 2
TOK_DEV = 256
STRING_LENGTH = 8192
EXPERTS = 32
CAP = 24
N_SP = 32
N_TP = 16


def decay_field(key, channels):
    keys = jax.random.split(key, 7)
    share = 0.5
    rapid_toggle = jax.random.bernoulli(keys[0], share, (2, 1, channels))
    quick = jax.random.uniform(keys[1], (2, 1, channels), jnp.float32, -0.5, 1.5)
    steady = math.log(STRING_LENGTH / 16.0) + jax.random.uniform(keys[2], (2, 1, channels), jnp.float32, 0.5, 1.5)
    floor_amount = jnp.where(rapid_toggle, quick, steady)
    spans = STRING_LENGTH // TOK_DEV
    additive_displacement = jnp.repeat(jax.random.uniform(keys[3], (2, spans, 1), jnp.float32, -0.7, 0.7), TOK_DEV, axis=1)
    jitter_magnitude = 0.7 * jax.random.truncated_normal(keys[4], -3.0, 3.0, (2, STRING_LENGTH, channels), jnp.float32)
    slot_numbers = jax.random.randint(keys[5], (2, 6), 0, STRING_LENGTH)
    sudden_jump = jnp.any(jnp.arange(STRING_LENGTH)[None, :, None] == slot_numbers[:, None, :], axis=2)[:, :, None]
    intensity_multiplier = jax.random.uniform(keys[6], (2, STRING_LENGTH, 1), jnp.float32, -11.0, -4.0)
    return jnp.where(sudden_jump & jnp.logical_not(rapid_toggle), intensity_multiplier, floor_amount + additive_displacement + jitter_magnitude).astype(jnp.float32)


def draw_decay_one(key, part):
    return decay_field(jax.random.fold_in(key, 11), HEADS_A * DK_A)


def draw_decay_two(key, part):
    return decay_field(jax.random.fold_in(key, 23), HEADS_B * DK_B)


def shard_levels(rng, shape, shards, smallest, high):
    level = 1.0
    for axis_at, shards_of in shards:
        heights = jax.random.uniform(jax.random.fold_in(jax.random.fold_in(rng, 6), axis_at), (shards_of,), jnp.float32, smallest / len(shards), high / len(shards))
        level = level * jnp.repeat(jnp.exp(heights), shape[axis_at] // shards_of).reshape((-1,) + (1,) * (len(shape) - 1 - axis_at))
    return level


def routed_block(stream_key, own, number, rows, count, top, bound, slope):
    ranking = jax.random.permutation(stream_key, count)
    packed, common = shares(count, rows * top, bound, slope, True), shares(count, rows * top, bound, slope, False)
    places = jnp.arange(count)

    def named(tallies, turn):
        used = int((tallies > 0).sum())
        fixed = max(1, used // 4)
        moved = fixed + (places - fixed + turn * (used - fixed)) % max(1, count - fixed)
        return jnp.zeros((count,), jnp.int32).at[ranking[jnp.where(places < fixed, places, moved)]].set(jnp.asarray(tallies, jnp.int32))

    tallies = jnp.where(number % 4 == 0, named(packed, number // 4), named(common, number - number // 4 - 1))
    mixed = jax.random.permutation(jax.random.fold_in(own, 3), count)
    donor, receiver = mixed[0:count // 2 * 2:2], mixed[1:count // 2 * 2:2]
    margin = jnp.minimum(tallies[donor] - 1, bound - tallies[receiver]) // 2
    margin = jnp.where((donor == ranking[0]) | (receiver == ranking[0]) | (tallies[receiver] == 0), 0, jnp.maximum(margin, 0))
    moved = jax.random.randint(jax.random.fold_in(own, 4), (count // 2,), 0, 1 << 20) % (margin + 1)
    tallies = tallies.at[donor].add(-moved).at[receiver].add(moved)
    labels = jnp.searchsorted(jnp.cumsum(tallies), jnp.arange(rows * top), side="right").astype(jnp.int32)
    listing = labels.reshape(top, rows).T
    listing = listing[jax.random.permutation(jax.random.fold_in(own, 1), rows)]
    turn = jax.random.randint(jax.random.fold_in(own, 2), (rows, 1), 0, top)
    return jnp.take_along_axis(listing, (jnp.arange(top)[None, :] + turn) % top, axis=1)


def shares(amount, total, bound, slope, full):
    loads = [(1 << 20) // math.isqrt(rank ** slope) + 1 for rank in range(1, amount + 1)]
    largest = bound if full else min(bound, max(-(-total // amount), total * loads[0] // sum(loads)))
    least = 1 if total - largest >= amount - 1 else 0
    given, rest = [largest] + [least] * (amount - 1), total - largest - least * (amount - 1)
    while rest > 0:
        movable = [i for i in range(1, amount) if given[i] < largest] or [i for i in range(1, amount) if given[i] < bound]
        pool, left = sum([loads[i] for i in movable]), rest
        for i in movable:
            addition = min(bound - given[i], max(1, left * loads[i] // pool), rest)
            given[i] = given[i] + addition
            rest = rest - addition
    return np.array(given)


def centred(own_key, extent, scale, limit, pieces=(), kind=jnp.bfloat16):
    values = jax.random.normal(own_key, extent, jnp.float32) * scale
    if len(pieces) > 0:
        values = shard_levels(own_key, extent, pieces, -0.22, 0.18) * values
    return jnp.clip(values, min=-limit, max=limit).astype(kind)


def setup_inputs(seed: int = 0) -> dict:
    seeds = jax.random.split(jax.random.key(seed), 22)
    query_one = centred(seeds[0], (STRING_LENGTH, HEADS_A * DK_A), 1.0, 6.0, ((0, 32), (1, 16)))
    key_one = centred(seeds[1], (STRING_LENGTH, HEADS_A * DK_A), 1.0, 6.0, ((0, 32), (1, 16)))
    value_one = centred(seeds[2], (STRING_LENGTH, HEADS_A * DV), 1.0, 6.0, ((0, 32), (1, 16)))
    gate_one = centred(seeds[3], (STRING_LENGTH, HEADS_A * DV), 1.0, 6.0, ((0, 32), (1, 16)))
    decay_one = draw_decay_one(jax.random.fold_in(seeds[21], 71), 0)
    query_two = centred(seeds[5], (STRING_LENGTH, HEADS_B * DK_B), 1.0, 6.0, ((0, 32), (1, 16)))
    key_two = centred(seeds[6], (STRING_LENGTH, HEADS_B * DK_B), 1.0, 6.0, ((0, 32), (1, 16)))
    value_two = centred(seeds[7], (STRING_LENGTH, HEADS_B * DV), 1.0, 6.0, ((0, 32), (1, 16)))
    gate_two = centred(seeds[8], (STRING_LENGTH, HEADS_B * DV), 1.0, 6.0, ((0, 32), (1, 16)))
    decay_two = draw_decay_two(jax.random.fold_in(seeds[21], 71), 0)
    head_gain = jnp.clip(1.0 + 0.18 * jax.random.normal(seeds[10], (DV,), jnp.float32), 0.1, 1.9)
    proj_one = centred(seeds[11], (HEADS_A * DV, D), ((HEADS_A + HEADS_B) * DV) ** -0.5, 0.09375, ((0, 16),))
    proj_two = centred(seeds[12], (HEADS_B * DV, D), ((HEADS_A + HEADS_B) * DV) ** -0.5, 0.09375, ((0, 16),))
    stream = centred(seeds[13], (STRING_LENGTH, D), 1.0, 6.0, ((0, 32),))
    gain_mix = jnp.clip(1.0 + 0.18 * jax.random.normal(seeds[14], (D,), jnp.float32), 0.1, 1.9)
    gain_moe = jnp.clip(1.0 + 0.18 * jax.random.normal(seeds[15], (D,), jnp.float32), 0.1, 1.9)
    routes_keys = jax.random.split(jax.random.fold_in(seeds[16], 1), STRING_LENGTH // TOK_DEV)
    routes_turns = jax.random.permutation(jax.random.fold_in(seeds[16], 3), STRING_LENGTH // TOK_DEV)
    routes = jax.vmap(lambda own, number: routed_block(jax.random.fold_in(seeds[16], 2), own, number, TOK_DEV, EXPERTS, TOPK, CAP, 2))(routes_keys, routes_turns).reshape((STRING_LENGTH, TOPK))
    affinity = jnp.clip(0.1 + 0.9 * jax.random.uniform(seeds[17], (STRING_LENGTH, TOPK), jnp.float32) ** shard_levels(seeds[17], (STRING_LENGTH, TOPK), ((0, 32),), -0.2, 0.2), 0.1, 1.0)
    expert_gate = centred(seeds[18], (EXPERTS, D, FF_E), D ** -0.5, 0.125, ((0, 32), (2, 16)))
    expert_up = centred(seeds[19], (EXPERTS, D, FF_E), D ** -0.5, 0.125, ((0, 32), (2, 16)))
    expert_down = centred(seeds[20], (EXPERTS, FF_E, D), FF_E ** -0.5, 0.125, ((0, 32), (1, 16)))
    return {"query_one": query_one, "key_one": key_one, "value_one": value_one, "gate_one": gate_one, "decay_one": decay_one, "query_two": query_two, "key_two": key_two, "value_two": value_two, "gate_two": gate_two, "decay_two": decay_two, "head_gain": head_gain, "proj_one": proj_one, "proj_two": proj_two, "stream": stream, "gain_mix": gain_mix, "gain_moe": gain_moe, "routes": routes, "affinity": affinity, "expert_gate": expert_gate, "expert_up": expert_up, "expert_down": expert_down}


normalizer_sharpness = 16.0
highest = lax.Precision.HIGHEST

def heads_first(values, heads):
    return values.reshape(values.shape[0], heads, -1).transpose(1, 0, 2)

def block_scan(query, key, value, logarithm_fading):
    heads, length, key_size = query.shape
    value_size = value.shape[-1]
    count = length // BLK

    def blocks(tensor):
        return tensor.reshape(heads, count, BLK, tensor.shape[-1])
    qb, kb, vb, gb = (blocks(query), blocks(key), blocks(value), blocks(logarithm_fading))
    cum = jnp.cumsum(gb, axis=2)
    last = cum[:, :, -1:, :]
    q_in = qb * jnp.exp(cum)
    k_in = kb * jnp.exp(-cum)
    k_st = kb * jnp.exp(last - cum)
    lower = jnp.tril(jnp.ones((BLK, BLK), dtype=bool))
    scores = jnp.where(lower, jnp.einsum('hnid,hnjd->hnij', q_in, k_in, precision=highest), 0.0)
    inner = jnp.einsum('hnij,hnjv->hniv', scores, vb, precision=highest)
    growth = jnp.einsum('hnjd,hnjv->hndv', k_st, vb, precision=highest)
    fading_speed = jnp.exp(last[:, :, 0, :])

    def step(state, inputs):
        factor, added = inputs
        return (factor[..., None] * state + added, state)
    final, starts = lax.scan(step, jnp.zeros((heads, key_size, value_size), jnp.float32), (fading_speed.transpose(1, 0, 2), growth.transpose(1, 0, 2, 3)))
    carried = jnp.einsum('hnid,hndv->hniv', q_in, starts.transpose(1, 0, 2, 3), precision=highest)
    return ((inner + carried).reshape(heads, length, value_size), final)

def group_mixed(query, key, value, fading_speed, key_size):
    heads = query.shape[1] // key_size
    qh = heads_first(query.astype(jnp.float32), heads) * key_size ** (-0.5)
    kh = heads_first(key.astype(jnp.float32), heads)
    vh = heads_first(value.astype(jnp.float32), heads)
    logarithm_fading = jax.nn.log_sigmoid(fading_speed) / normalizer_sharpness
    ahead = heads_first(logarithm_fading[0], heads)
    behind = heads_first(logarithm_fading[1], heads)
    forward, _ = block_scan(qh, kh, vh, ahead)
    backward, _ = block_scan(qh[:, ::-1], kh[:, ::-1], vh[:, ::-1], behind[:, ::-1])
    return forward + backward[:, ::-1]

def finish(mixed, gate, head_gain):
    normed = mixed * lax.rsqrt(lax.optimization_barrier(jnp.mean(mixed * mixed, axis=-1, keepdims=True)) + 1e-06) * head_gain
    flat = normed.transpose(1, 0, 2).reshape(mixed.shape[1], -1)
    return (flat * jax.nn.silu(gate.astype(jnp.float32))).astype(jnp.bfloat16)

def layer_norm(values, gain):
    mean = lax.optimization_barrier(jnp.mean(values, axis=-1, keepdims=True))
    spread = lax.optimization_barrier(jnp.mean(jnp.square(values - mean), axis=-1, keepdims=True))
    return (values - mean) * lax.rsqrt(spread + 1e-05) * gain

def reference(query_one, key_one, value_one, gate_one, decay_one, query_two, key_two, value_two, gate_two, decay_two, head_gain, proj_one, proj_two, stream, gain_mix, gain_moe, routes, affinity, expert_gate, expert_up, expert_down):
    heads_one = finish(group_mixed(query_one, key_one, value_one, decay_one, DK_A), gate_one, head_gain)
    heads_two = finish(group_mixed(query_two, key_two, value_two, decay_two, DK_B), gate_two, head_gain)
    width_one = HEADS_A // N_TP * DV
    width_two = HEADS_B // N_TP * DV
    total = jnp.zeros((STRING_LENGTH, D), jnp.float32)
    for block in range(N_TP):
        part = jnp.dot(heads_one[:, block * width_one:(block + 1) * width_one], proj_one[block * width_one:(block + 1) * width_one], preferred_element_type=jnp.float32)
        part = part + jnp.dot(heads_two[:, block * width_two:(block + 1) * width_two], proj_two[block * width_two:(block + 1) * width_two], preferred_element_type=jnp.float32)
        total = total + lax.optimization_barrier(part.astype(jnp.bfloat16)).astype(jnp.float32)
    attn = total.astype(jnp.bfloat16)
    settled = layer_norm(stream.astype(jnp.float32) + attn.astype(jnp.float32), gain_mix)
    moe_in = settled.astype(jnp.bfloat16)
    weights = (affinity / lax.optimization_barrier(jnp.sum(affinity, axis=-1, keepdims=True))).reshape(-1)
    assigned = STRING_LENGTH * TOPK
    flat_expert = routes.reshape(-1).astype(jnp.int32)
    order = jnp.argsort(flat_expert, stable=True).astype(jnp.int32)
    sorted_expert = flat_expert[order]
    counts = lax.optimization_barrier(jnp.sum((flat_expert[:, None] == jnp.arange(EXPERTS, dtype=jnp.int32)[None, :]).astype(jnp.int32), axis=0)).astype(jnp.int32)
    starts = (jnp.cumsum(counts).astype(jnp.int32) - counts).astype(jnp.int32)
    most_rows = N_SP * CAP
    slot = (jnp.arange(assigned, dtype=jnp.int32) - starts[sorted_expert]).astype(jnp.int32)
    table = jnp.full((EXPERTS * most_rows,), -1, jnp.int32).at[sorted_expert * most_rows + slot].set(order)
    table = table.reshape(EXPERTS, most_rows)
    unit_block = FF_E // N_TP

    def per_expert(acc, expert):
        entries = table[expert]
        valid = entries >= 0
        safe = jnp.where(valid, entries, 0).astype(jnp.int32)
        token = (safe // TOPK).astype(jnp.int32)
        rows = moe_in[token]
        gate = jnp.dot(rows, expert_gate[expert], preferred_element_type=jnp.float32)
        upward = jnp.dot(rows, expert_up[expert], preferred_element_type=jnp.float32)
        act = (jax.nn.silu(gate) * upward).astype(jnp.bfloat16)
        act_blocks = act.astype(jnp.float32).reshape(most_rows, N_TP, unit_block)
        down_blocks = expert_down[expert].astype(jnp.float32).reshape(N_TP, unit_block, D)
        partial_value = jnp.einsum('rbf,bfd->rbd', act_blocks, down_blocks, precision=highest)
        rounded = lax.optimization_barrier(partial_value.astype(jnp.bfloat16)).astype(jnp.float32)
        piece = lax.optimization_barrier(lax.optimization_barrier(jnp.sum(rounded, axis=1)).astype(jnp.bfloat16)).astype(jnp.float32)
        scale = jnp.where(valid, weights[safe], 0.0)
        return (acc.at[token].add(scale[:, None] * piece), None)
    mixture, _ = lax.scan(per_expert, jnp.zeros((STRING_LENGTH, D), jnp.float32), jnp.arange(EXPERTS, dtype=jnp.int32))
    return layer_norm(settled + mixture, gain_moe).astype(jnp.bfloat16)
```

```python
import jax
import jax.numpy as jnp
from jax import lax
from jax.experimental import pallas as pl
from jax.experimental.pallas import tpu as pltpu
from jax.sharding import Mesh
from jax.sharding import PartitionSpec as P


DK_A = 64
DK_B = 128
BLK = 64
SHARERS = 4
SLOTS = 6
STEP = 16
SP = ("z", "x")
Y = ("p", "b")
TP = ("p", "b", "c")
ALL = ("z", "x", "p", "b", "c")
SWAP = [(0, 1), (1, 0)]
F32 = jnp.float32
BF16 = jnp.bfloat16
VMEM_LIMIT = 16 * 1024 * 1024
normalizer_sharpness = 16.0


def call(kernel, outs, *args, far=(), scratch=()):
    single = not isinstance(outs, (list, tuple))
    shapes = [outs] if single else list(outs)
    vmem = pl.BlockSpec(memory_space=pltpu.VMEM)
    smem = pl.BlockSpec(memory_space=pltpu.SMEM)
    found = pl.pallas_call(
        kernel,
        out_shape=shapes,
        in_specs=[
            pl.BlockSpec(memory_space=pltpu.HBM)
            if k in far
            else smem
            if arg.ndim == 1
            else vmem
            for k, arg in enumerate(args)
        ],
        out_specs=[vmem] * len(shapes),
        scratch_shapes=list(scratch),
        compiler_params=pltpu.CompilerParams(vmem_limit_bytes=VMEM_LIMIT),
    )(
        *(
            pltpu.with_memory_space_constraint(arg, pltpu.HBM) if k in far else arg
            for k, arg in enumerate(args)
        )
    )
    return found[0] if single else found


def fetched(sources, places, marks):
    copies = [
        pltpu.make_async_copy(source, place, marks.at[k])
        for k, (source, place) in enumerate(zip(sources, places))
    ]
    for copy in copies:
        copy.start()
    return copies


def exact_dot(a, b, dims=((1,), (0,))):
    return lax.dot_general(
        a, b, (dims, ((), ())), precision=lax.Precision.HIGHEST, preferred_element_type=F32
    )


def fast_dot(a, b, dims=((1,), (0,))):
    return lax.dot_general(
        a.astype(BF16), b.astype(BF16), (dims, ((), ())), preferred_element_type=F32
    )


def log_fading(pre):
    return (jnp.minimum(pre, 0.0) - jnp.log1p(jnp.exp(-jnp.abs(pre)))) / normalizer_sharpness


def grid_of(length):
    row = lax.broadcasted_iota(jnp.int32, (length, length), 0)
    col = lax.broadcasted_iota(jnp.int32, (length, length), 1)
    return row, col


def states_kernel(
    d1h, d2h, k1h, v1h, k2h, v2h, gate, up, down, one, two,
    pieces, pack, proj,
    d1, d2, k1, v1, k2, v2, spread, marks, moves,
):
    copies = fetched((d1h, d2h, k1h, v1h, k2h, v2h), (d1, d2, k1, v1, k2, v2), marks)
    features, hidden = gate.shape[1:]
    blocks = down.shape[2] // (2 * hidden)
    sources = [gate.at[0], up.at[0], one, two]
    places = [
        pack.at[:features, :hidden],
        pack.at[:features, hidden:],
        proj.at[:hidden, :],
        proj.at[hidden:, :],
    ]
    for n in range(blocks):
        sources.append(down.at[0, :, 2 * hidden * n : 2 * hidden * (n + 1)])
        places.append(pack.at[features + hidden * n : features + hidden * (n + 1), :])
    moved = fetched(sources, places, moves)
    size, length = k1.shape
    peers = spread.shape[0] // 24
    row, col = grid_of(length)
    above = (row < col).astype(F32)
    below = (row > col).astype(F32)
    ones = jnp.ones((length, 128), F32)

    def put(value, kind, first):
        for n in range(value.shape[0] // peers):
            spread[pl.ds(kind * 6 + first + n, peers, stride=24), :] = value[
                n * peers : (n + 1) * peers
            ]

    copies[0].wait()
    ahead, behind = log_fading(d1[0]), log_fading(d1[1])
    fade_f = jnp.exp(exact_dot(ahead, below))
    fade_b = jnp.exp(exact_dot(behind, above))
    put(exact_dot(ahead, ones), 2, 0)
    put(exact_dot(behind, ones), 3, 0)
    copies[1].wait()
    ahead, behind = log_fading(d2[0]), log_fading(d2[1])
    wide_f = jnp.exp(exact_dot(above, ahead))
    wide_b = jnp.exp(exact_dot(below, behind))
    across = ((0,), (0,))
    put(exact_dot(ahead, ones, across), 2, size // peers)
    put(exact_dot(behind, ones, across), 3, size // peers)
    copies[2].wait()
    copies[3].wait()
    key, value = k1[...].astype(F32), v1[...]
    put(fast_dot(key * fade_f, value), 0, 0)
    put(fast_dot(key * fade_b, value), 1, 0)
    copies[4].wait()
    copies[5].wait()
    key, value = k2[...].astype(F32), v2[...]
    put(fast_dot(key * wide_f, value, across), 0, size // peers)
    put(fast_dot(key * wide_b, value, across), 1, size // peers)
    pieces[...] = spread[...].astype(BF16)
    for copy in moved:
        copy.wait()


def scan_kernel(pieces, out):
    peers, rows2, lanes = pieces.shape
    rows = rows2 // 2
    half = rows // 2
    forward = lax.broadcasted_iota(jnp.int32, (rows, lanes), 0) < half
    state = jnp.zeros((rows, lanes), F32)
    found = []
    for place in range(peers):
        found.append(state)
        if place + 1 < peers:
            whole = pieces[place].astype(F32)
            state = jnp.exp(whole[rows:]) * state + whole[:rows]
    state = jnp.zeros((rows, lanes), F32)
    for place in reversed(range(peers)):
        out[place, :rows] = jnp.where(forward, found[place], state).astype(BF16)
        out[place, rows:] = jnp.zeros((out.shape[1] - rows, lanes), BF16)
        if place > 0:
            whole = pieces[place].astype(F32)
            state = jnp.exp(whole[rows:]) * state + whole[:rows]


def local_kernel(
    q1h, k1h, v1h, d1h, q2h, k2h, v2h, d2h, g1h, g2h, gain,
    mixed, reader_one, reader_two, opened,
    q1, k1, v1, d1, q2, k2, v2, d2, g1, g2, marks,
):
    copies = fetched(
        (q1h, k1h, v1h, d1h, q2h, k2h, v2h, d2h, g1h, g2h),
        (q1, k1, v1, d1, q2, k2, v2, d2, g1, g2),
        marks,
    )
    for copy in copies:
        copy.wait()
    length = v1.shape[0]
    for place, gate in enumerate((g1, g2)):
        value = gate[...].astype(F32)
        opened[:, place * 128 : (place + 1) * 128] = value * jax.nn.sigmoid(value) * gain[...]
    count = length // BLK
    row, col = grid_of(length)
    upto = (col <= row).astype(F32)
    since = (col >= row).astype(F32)
    brow, bcol = grid_of(BLK)
    lower, upper = bcol <= brow, bcol >= brow
    on_last = ((1,), (1,))
    at = 0
    for q_ref, k_ref, v_ref, d_ref, reader in (
        (q1, k1, v1, d1, reader_one),
        (q2, k2, v2, d2, reader_two),
    ):
        size = reader.shape[1] // 2
        query = q_ref[...].astype(F32) * size ** (-0.5)
        key = k_ref[...].astype(F32)
        value = v_ref[...]
        ahead, behind = d_ref[0], d_ref[1]
        if size == DK_A:
            query, key, ahead, behind = query.T, key.T, ahead.T, behind.T
        ahead, behind = log_fading(ahead), log_fading(behind)
        cum_f = exact_dot(upto, ahead)
        cum_b = exact_dot(since, behind)
        reader[:, :size] = (query * jnp.exp(cum_f)).astype(BF16)
        reader[:, size:] = (query * jnp.exp(cum_b)).astype(BF16)
        sums = []
        for i in range(count):
            part = slice(i * BLK, (i + 1) * BLK)
            own_f, own_b = ahead[part], behind[part]
            local_f = exact_dot(upto[:BLK, :BLK], own_f)
            local_b = exact_dot(since[:BLK, :BLK], own_b)
            q_i, k_i = query[part], key[part]
            score_f = fast_dot(q_i * jnp.exp(local_f), k_i * jnp.exp(-local_f), on_last)
            score_b = fast_dot(q_i * jnp.exp(local_b), k_i * jnp.exp(-local_b), on_last)
            score = jnp.where(lower, score_f, 0.0) + jnp.where(upper, score_b, 0.0)
            sums.append(fast_dot(score, value[part]))
        for j in range(count):
            part = slice(j * BLK, (j + 1) * BLK)
            if j + 1 < count:
                rest = slice((j + 1) * BLK, length)
                end = cum_f[(j + 1) * BLK - 1 : (j + 1) * BLK]
                gone = fast_dot(
                    query[rest] * jnp.exp(cum_f[rest] - end),
                    key[part] * jnp.exp(end - cum_f[part]),
                    on_last,
                )
                carried = fast_dot(gone, value[part])
                for i in range(j + 1, count):
                    sums[i] = sums[i] + carried[(i - j - 1) * BLK : (i - j) * BLK]
            if j > 0:
                rest = slice(0, j * BLK)
                end = cum_b[j * BLK : j * BLK + 1]
                gone = fast_dot(
                    query[rest] * jnp.exp(cum_b[rest] - end),
                    key[part] * jnp.exp(end - cum_b[part]),
                    on_last,
                )
                carried = fast_dot(gone, value[part])
                for i in range(j):
                    sums[i] = sums[i] + carried[i * BLK : (i + 1) * BLK]
        for i in range(count):
            mixed[i * BLK : (i + 1) * BLK, at : at + 128] = sums[i]
        at += 128


def heads_kernel(
    core, local, reader_one, reader_two, carried, opened, own, sent, both, spread
):
    width = 128
    length = local.shape[0]
    spread[...] = carried[...].astype(F32)
    peers = spread.shape[0] // 16

    def state(first, last):
        return jnp.concatenate(
            [
                spread[pl.ds(kind * 6 + n, peers, stride=16), :]
                for kind in range(2)
                for n in range(first, last)
            ],
            axis=0,
        )

    at = 0
    for reader, held in ((reader_one, state(0, 2)), (reader_two, state(2, 6))):
        mixed = local[:, at : at + width] + fast_dot(reader[...], held)
        scale = lax.rsqrt(jnp.mean(mixed * mixed, axis=-1, keepdims=True) + 1e-06)
        heads = (mixed * scale * opened[:, at : at + width]).astype(BF16)
        for turn in range(length // STEP):
            where = (turn // 2) * STEP
            both[turn % 2, where : where + STEP, at : at + width] = heads[
                turn * STEP : (turn + 1) * STEP
            ]
        at += width
    own[...] = both[core[0]]
    sent[...] = both[1 - core[0]]


def routing_kernel(where, routes, affinity, chosen, weighted):
    core, first = where[0], where[1]
    rows = routes.shape[1]
    slots = chosen.shape[0]
    experts = slots // SLOTS
    half = rows // 2
    row, col = grid_of(rows)
    inner = lax.rem(row, half)
    turn = jnp.where(row < half, core, 1 - core)
    token = 2 * STEP * lax.div(inner, STEP) + STEP * turn + lax.rem(inner, STEP)
    order = (token == col).astype(F32)
    lane = lax.broadcasted_iota(jnp.int32, (experts, rows), 0)
    named = [routes[k : k + 1, :] for k in range(2)]
    hot = [(lane == name).astype(F32) for name in named]
    before = fast_dot(hot[0] + hot[1], (row < col).astype(BF16))
    share = affinity[...]
    share = share / jnp.sum(share, axis=0, keepdims=True)
    lines = []
    for k in range(2):
        rank = jnp.sum(hot[k] * before, axis=0, keepdims=True).astype(jnp.int32) - first
        inside = (rank >= 0) & (rank < SLOTS)
        spot = jnp.where(inside, rank * experts + named[k], -1)
        lines.append(spot.astype(F32))
    lines += [share[0:1, :], share[1:2, :]]
    lines = jnp.concatenate(lines + [jnp.zeros((4, rows), F32)], axis=0)
    flat = exact_dot(lines, order, ((1,), (1,)))
    tall = exact_dot(order, lines, ((1,), (1,)))
    place = lax.broadcasted_iota(jnp.int32, (slots, rows), 0).astype(F32)
    hit = (place == flat[0:1, :]) | (place == flat[1:2, :])
    chosen[...] = hit.astype(F32).astype(BF16)
    place = lax.broadcasted_iota(jnp.int32, (rows, slots), 1).astype(F32)
    scaled = jnp.where(place == tall[:, 0:1], tall[:, 2:3], 0.0)
    scaled = scaled + jnp.where(place == tall[:, 1:2], tall[:, 3:4], 0.0)
    weighted[...] = scaled.astype(BF16)


def loosen(packed, spread):
    for n in range(spread.shape[0]):
        spread[n] = packed[:, n * 128 : (n + 1) * 128].astype(F32)


def tighten(spread, packed):
    for n in range(spread.shape[0]):
        packed[:, n * 128 : (n + 1) * 128] = spread[n].astype(BF16)


def strided(part, slot, peers):
    return pl.ds(part * SLOTS + slot, peers, stride=SHARERS * SLOTS)


def taken(spread, part):
    peers = spread.shape[1] // (SHARERS * SLOTS)
    return jnp.concatenate(
        [
            jnp.concatenate(
                [spread[n, strided(part, slot, peers), :] for slot in range(SLOTS)], axis=0
            ).astype(BF16)
            for n in range(spread.shape[0])
        ],
        axis=1,
    )


def placed(spread, part, value, lane):
    peers = spread.shape[1] // (SHARERS * SLOTS)
    for n in range(value.shape[1] // 128):
        for slot in range(SLOTS):
            spread[lane + n, strided(part, slot, peers), :] = value[
                slot * peers : (slot + 1) * peers, n * 128 : (n + 1) * 128
            ]


def dispatch_kernel(chosen, own, other, out, spread):
    wide = out.shape[1]
    for part in range(SHARERS):
        lanes = slice(part * wide, (part + 1) * wide)
        both = jnp.concatenate([own[:, lanes], other[:, lanes]], axis=0)
        placed(spread, part, fast_dot(chosen[...], both), 0)
    tighten(spread, out)


def expert_kernel(rows, own, near, side, far, out, spread):
    wide = rows.shape[1]
    hidden = own.shape[1] // 2
    packs = (own, near, side, far)
    loosen(rows, spread)
    x = jnp.concatenate([taken(spread, part) for part in range(SHARERS)], axis=1)
    features = SHARERS * wide
    acts = []
    for pack in packs:
        both = fast_dot(x, pack[:features, :])
        gate, upward = both[:, :hidden], both[:, hidden:]
        acts.append((gate * jax.nn.sigmoid(gate) * upward).astype(BF16))
    acts = [jnp.concatenate(acts[:2], axis=1), jnp.concatenate(acts[2:], axis=1)]
    step = 2 * hidden
    for n in range(features // step):
        here = slice(features + n * hidden, features + (n + 1) * hidden)
        value = 0.0
        for act, pair in zip(acts, (packs[:2], packs[2:])):
            value = value + fast_dot(act, jnp.concatenate([pack[here, :] for pack in pair], axis=0))
        placed(spread, n * step // wide, value, n * step % wide // 128)
    tighten(spread, out)


def combine_kernel(weighted, returned, own, sent, spread):
    half = own.shape[0]
    wide = returned.shape[1]
    loosen(returned, spread)
    for part in range(SHARERS):
        value = fast_dot(weighted[...], taken(spread, part))
        own[:, part * wide : (part + 1) * wide] = value[:half]
        sent[:, part * wide : (part + 1) * wide] = value[half:].astype(BF16)


def settle_kernel(parts, stream, gain, settled, copies):
    total = 0.0
    for place in range(parts.shape[0]):
        total = total + parts[place].astype(F32)
    attn = total.astype(BF16).astype(F32)
    found = layer_norm(stream[...].astype(F32) + attn, gain[...])
    settled[...] = found
    for place in range(parts.shape[0]):
        copies[place] = found.astype(BF16)


def finish_kernel(parts, settled, gain, out):
    total = 0.0
    for place in range(parts.shape[0]):
        total = total + parts[place].astype(F32)
    out[...] = layer_norm(settled[...] + total, gain[...]).astype(BF16)


def join_kernel(own, got, out):
    out[...] = (own[...] + got[...].astype(F32)).astype(BF16)


def project_kernel(own, got, proj, other, out):
    width = out.shape[1]
    step = width // 4
    for n in range(4):
        lanes = slice(n * step, (n + 1) * step)
        value = fast_dot(own[...], proj[:, lanes]) + fast_dot(got[...], other[:, lanes])
        out[:, lanes] = value.astype(BF16)


def layer_norm(values, gain):
    mean = jnp.mean(values, axis=-1, keepdims=True)
    spread = jnp.mean(jnp.square(values - mean), axis=-1, keepdims=True)
    return (values - mean) * lax.rsqrt(spread + 1e-05) * gain


def exchange(pieces, axis):
    return lax.all_to_all(pieces, axis, split_axis=0, concat_axis=0, tiled=True)


def swapped(value, axis):
    return lax.ppermute(value, axis, SWAP)


def tied(value, after):
    return lax.optimization_barrier((value, after))[0]


def body(
    query_one,
    key_one,
    value_one,
    gate_one,
    decay_one,
    query_two,
    key_two,
    value_two,
    gate_two,
    decay_two,
    head_gain,
    proj_one,
    proj_two,
    stream,
    gain_mix,
    gain_moe,
    routes,
    affinity,
    expert_gate,
    expert_up,
    expert_down,
):
    return layer(
        query_one.T,
        key_one.T,
        value_one,
        gate_one,
        jnp.swapaxes(decay_one, 1, 2),
        query_two,
        key_two,
        value_two,
        gate_two,
        decay_two,
        head_gain,
        proj_one,
        proj_two,
        stream,
        gain_mix,
        gain_moe,
        routes,
        affinity,
        expert_gate,
        expert_up,
        expert_down,
    )


def layer(
    query_one,
    key_one,
    value_one,
    gate_one,
    decay_one,
    query_two,
    key_two,
    value_two,
    gate_two,
    decay_two,
    head_gain,
    proj_one,
    proj_two,
    stream,
    gain_mix,
    gain_moe,
    routes,
    affinity,
    expert_gate,
    expert_up,
    expert_down,
):
    rows = query_two.shape[0]
    width = stream.shape[1]
    peers = lax.axis_size(SP)
    chips = lax.axis_size(Y)
    tp_count = lax.axis_size(TP)
    own_rows = rows // tp_count
    half = rows // 2
    core = lax.axis_index("c")
    tp_rank = lax.axis_index(TP)
    group = lax.axis_index(("b", "c"))
    hidden = expert_gate.shape[2]
    slots = peers * SLOTS
    total = SHARERS * slots
    wide = width // SHARERS
    keys = DK_A + DK_B
    shape = jax.ShapeDtypeStruct

    def scratch(items):
        held = [pltpu.VMEM(item.shape, item.dtype) for item in items]
        return held, pltpu.SemaphoreType.DMA((len(items),))

    early = (decay_one, decay_two, key_one, value_one, key_two, value_two)
    moves = (expert_gate, expert_up, expert_down, proj_one, proj_two)
    held, marks = scratch(early)
    lines = 4 * keys
    blocks = width // (2 * hidden)
    pieces, pack, proj = call(
        states_kernel,
        [
            pltpu.HBM((lines, 128), BF16),
            shape((width + blocks * hidden, 2 * hidden), BF16),
            shape((2 * hidden, width), BF16),
        ],
        *early,
        *moves,
        far=range(len(early) + len(moves)),
        scratch=held
        + [pltpu.VMEM((lines, 128), F32), marks, pltpu.SemaphoreType.DMA((4 + blocks,))],
    )
    pieces = pieces.reshape(peers, lines // peers, 128)
    near = swapped(pack, "b")
    side = swapped(pack, "c")
    proj_other = swapped(proj, "c")
    arrived = exchange(pieces, SP)
    late = (
        query_one,
        key_one,
        value_one,
        decay_one,
        query_two,
        key_two,
        value_two,
        decay_two,
        gate_one,
        gate_two,
    )
    held, marks = scratch(late)
    local, reader_one, reader_two, opened = call(
        local_kernel,
        [
            shape((rows, 256), F32),
            shape((rows, 2 * DK_A), BF16),
            shape((rows, 2 * DK_B), BF16),
            shape((rows, 256), F32),
        ],
        *late,
        head_gain.reshape(1, 128),
        far=range(len(late)),
        scratch=held + [marks],
    )
    chosen, weighted = call(
        routing_kernel,
        [shape((slots, rows), BF16), shape((rows, slots), BF16)],
        jnp.stack([core, group * SLOTS]).astype(jnp.int32),
        routes.T,
        affinity.T,
    )
    starts = call(
        scan_kernel, pltpu.HBM((peers, 16, 128), BF16), arrived
    )
    carried = exchange(starts, SP).reshape(peers * 16, 128)
    heads_own, heads_sent = call(
        heads_kernel,
        [shape((half, 256), BF16)] * 2,
        core.reshape(1).astype(jnp.int32),
        local,
        reader_one,
        reader_two,
        carried,
        opened,
        scratch=[pltpu.VMEM((2, half, 256), BF16), pltpu.VMEM((peers * 16, 128), F32)],
    )
    far = swapped(tied(near, heads_own), "c")
    heads_got = swapped(heads_sent, "c")
    part = call(
        project_kernel, pltpu.HBM((half, width), BF16), heads_own, heads_got, proj, proj_other
    )
    attn = exchange(part.reshape(chips, own_rows, width), Y)
    stream_own = lax.dynamic_slice_in_dim(stream, tp_rank * own_rows, own_rows, 0)
    settled, mine = call(
        settle_kernel,
        [shape((own_rows, width), F32), pltpu.HBM((chips, own_rows, width), BF16)],
        attn,
        stream_own,
        gain_mix.reshape(1, width),
    )
    moe_own = exchange(mine, Y).reshape(half, width)
    moe_other = swapped(moe_own, "c")
    spread = [pltpu.VMEM((wide // 128, total, 128), F32)]
    outgoing = call(
        dispatch_kernel,
        pltpu.HBM((total, wide), BF16),
        chosen,
        moe_own,
        moe_other,
        scratch=spread,
    )
    complete = exchange(outgoing.reshape(peers, total // peers, wide), SP)
    partial = call(
        expert_kernel,
        pltpu.HBM((total, wide), BF16),
        complete.reshape(total, wide),
        pack,
        near,
        side,
        far,
        scratch=spread,
    )
    returned = exchange(partial.reshape(peers, total // peers, wide), SP)
    term_own, term_sent = call(
        combine_kernel,
        [shape((half, width), F32), shape((half, width), BF16)],
        weighted,
        returned.reshape(total, wide),
        scratch=spread,
    )
    term = call(join_kernel, pltpu.HBM((half, width), BF16), term_own, swapped(term_sent, "c"))
    mixture = exchange(term.reshape(chips, own_rows, width), Y)
    return call(
        finish_kernel,
        shape((own_rows, width), BF16),
        mixture,
        settled,
        gain_moe.reshape(1, width),
    )


def solution(mesh):
    finer = Mesh(mesh.devices.reshape(8, 4, 4, 2, 2), ALL)
    return jax.shard_map(
        body,
        mesh=finer,
        in_specs=(
            P(SP, TP),
            P(SP, TP),
            P(SP, TP),
            P(SP, TP),
            P(None, SP, TP),
            P(SP, TP),
            P(SP, TP),
            P(SP, TP),
            P(SP, TP),
            P(None, SP, TP),
            P(),
            P(TP, None),
            P(TP, None),
            P(SP, None),
            P(),
            P(),
            P(SP, None),
            P(SP, None),
            P(SP, None, TP),
            P(SP, None, TP),
            P(SP, TP, None),
        ),
        out_specs=P(ALL, None),
        check_vma=False,
    )
```

```python
import jax
import jax.numpy as jnp
from jax import lax
from jax.experimental import pallas as pl
from jax.experimental.pallas import tpu as pltpu
from jax.sharding import Mesh
from jax.sharding import PartitionSpec as P


DK_A = 64
DK_B = 128
BLK = 64
SHARERS = 4
SLOTS = 6
STEP = 16
SPLIT = 1
LINES = SHARERS * SLOTS
SP = ("z", "x")
Y = ("p", "b")
TP = ("p", "b", "c")
ALL = ("z", "x", "p", "b", "c")
SWAP = [(0, 1), (1, 0)]
F32 = jnp.float32
BF16 = jnp.bfloat16
VMEM_LIMIT = 32 * 1024 * 1024
normalizer_sharpness = 16.0


def call(kernel, outs, *args, far=(), scratch=()):
    single = not isinstance(outs, (list, tuple))
    shapes = [outs] if single else list(outs)
    vmem = pl.BlockSpec(memory_space=pltpu.VMEM)
    smem = pl.BlockSpec(memory_space=pltpu.SMEM)
    found = pl.pallas_call(
        kernel,
        out_shape=shapes,
        in_specs=[
            pl.BlockSpec(memory_space=pltpu.HBM)
            if k in far
            else smem
            if arg.ndim == 1
            else vmem
            for k, arg in enumerate(args)
        ],
        out_specs=[vmem] * len(shapes),
        scratch_shapes=list(scratch),
        compiler_params=pltpu.CompilerParams(vmem_limit_bytes=VMEM_LIMIT),
    )(
        *(
            pltpu.with_memory_space_constraint(arg, pltpu.HBM) if k in far else arg
            for k, arg in enumerate(args)
        )
    )
    return found[0] if single else found


def fetched(sources, places, marks):
    copies = [
        pltpu.make_async_copy(source, place, marks.at[k])
        for k, (source, place) in enumerate(zip(sources, places))
    ]
    for copy in copies:
        copy.start()
    return copies


def exact_dot(a, b, dims=((1,), (0,))):
    return lax.dot_general(
        a, b, (dims, ((), ())), precision=lax.Precision.HIGHEST, preferred_element_type=F32
    )


def fast_dot(a, b, dims=((1,), (0,))):
    return lax.dot_general(
        a.astype(BF16), b.astype(BF16), (dims, ((), ())), preferred_element_type=F32
    )


def log_fading(pre):
    return (jnp.minimum(pre, 0.0) - jnp.log1p(jnp.exp(-jnp.abs(pre)))) / normalizer_sharpness


def grid_of(length):
    row = lax.broadcasted_iota(jnp.int32, (length, length), 0)
    col = lax.broadcasted_iota(jnp.int32, (length, length), 1)
    return row, col


def states_kernel(
    d1h, d2h, k1h, v1h, k2h, v2h, pieces, d1, d2, k1, v1, k2, v2, spread, marks
):
    copies = fetched((d1h, d2h, k1h, v1h, k2h, v2h), (d1, d2, k1, v1, k2, v2), marks)
    size, length = k1.shape
    peers = spread.shape[0] // 24
    row, col = grid_of(length)
    above = (row < col).astype(F32)
    below = (row > col).astype(F32)
    ones = jnp.ones((length, 128), F32)

    def put(value, kind, first):
        for n in range(value.shape[0] // peers):
            spread[pl.ds(kind * 6 + first + n, peers, stride=24), :] = value[
                n * peers : (n + 1) * peers
            ]

    copies[0].wait()
    ahead, behind = log_fading(d1[0]), log_fading(d1[1])
    fade_f = jnp.exp(exact_dot(ahead, below))
    fade_b = jnp.exp(exact_dot(behind, above))
    put(exact_dot(ahead, ones), 2, 0)
    put(exact_dot(behind, ones), 3, 0)
    copies[1].wait()
    ahead, behind = log_fading(d2[0]), log_fading(d2[1])
    wide_f = jnp.exp(exact_dot(above, ahead))
    wide_b = jnp.exp(exact_dot(below, behind))
    across = ((0,), (0,))
    put(exact_dot(ahead, ones, across), 2, size // peers)
    put(exact_dot(behind, ones, across), 3, size // peers)
    copies[2].wait()
    copies[3].wait()
    key, value = k1[...].astype(F32), v1[...]
    put(fast_dot(key * fade_f, value), 0, 0)
    put(fast_dot(key * fade_b, value), 1, 0)
    copies[4].wait()
    copies[5].wait()
    key, value = k2[...].astype(F32), v2[...]
    put(fast_dot(key * wide_f, value, across), 0, size // peers)
    put(fast_dot(key * wide_b, value, across), 1, size // peers)
    pieces[...] = spread[...].astype(BF16)


def pack_kernel(where, gate, up, down, one, two, stream, pack, proj, own, moves):
    features, hidden = gate.shape[1:]
    sources = [gate.at[0], up.at[0], one, two]
    places = [
        pack.at[:features, :hidden],
        pack.at[:features, hidden:],
        proj.at[:hidden, :],
        proj.at[hidden:, :],
    ]
    for n in range(down.shape[2] // (2 * hidden)):
        sources.append(down.at[0, :, 2 * hidden * n : 2 * hidden * (n + 1)])
        places.append(pack.at[features + hidden * n : features + hidden * (n + 1), :])
    rows = own.shape[0]
    sources.append(stream.at[pl.ds(pl.multiple_of(where[0] * rows, rows), rows), :])
    places.append(own)
    for copy in fetched(sources, places, moves):
        copy.wait()


def scan_kernel(pieces, out):
    peers, rows2, lanes = pieces.shape
    rows = rows2 // 2
    half = rows // 2
    forward = lax.broadcasted_iota(jnp.int32, (rows, lanes), 0) < half
    state = jnp.zeros((rows, lanes), F32)
    found = []
    for place in range(peers):
        found.append(state)
        if place + 1 < peers:
            whole = pieces[place].astype(F32)
            state = jnp.exp(whole[rows:]) * state + whole[:rows]
    state = jnp.zeros((rows, lanes), F32)
    for place in reversed(range(peers)):
        out[place, :rows] = jnp.where(forward, found[place], state).astype(BF16)
        out[place, rows:] = jnp.zeros((out.shape[1] - rows, lanes), BF16)
        if place > 0:
            whole = pieces[place].astype(F32)
            state = jnp.exp(whole[rows:]) * state + whole[:rows]


def local_kernel(
    q1h, k1h, v1h, d1h, q2h, k2h, v2h, d2h, g1h, g2h, gain,
    mixed, reader_one, reader_two, opened,
    q1, k1, v1, d1, q2, k2, v2, d2, g1, g2, marks,
):
    copies = fetched(
        (q1h, k1h, v1h, d1h, q2h, k2h, v2h, d2h, g1h, g2h),
        (q1, k1, v1, d1, q2, k2, v2, d2, g1, g2),
        marks,
    )
    for copy in copies:
        copy.wait()
    length = v1.shape[0]
    for place, gate in enumerate((g1, g2)):
        value = gate[...].astype(F32)
        opened[:, place * 128 : (place + 1) * 128] = value * jax.nn.sigmoid(value) * gain[...]
    count = length // BLK
    row, col = grid_of(length)
    upto = (col <= row).astype(F32)
    since = (col >= row).astype(F32)
    brow, bcol = grid_of(BLK)
    lower, upper = bcol <= brow, bcol >= brow
    on_last = ((1,), (1,))
    at = 0
    for q_ref, k_ref, v_ref, d_ref, reader in (
        (q1, k1, v1, d1, reader_one),
        (q2, k2, v2, d2, reader_two),
    ):
        size = reader.shape[1] // 2
        query = q_ref[...].astype(F32) * size ** (-0.5)
        key = k_ref[...].astype(F32)
        value = v_ref[...]
        ahead, behind = d_ref[0], d_ref[1]
        if size == DK_A:
            query, key, ahead, behind = query.T, key.T, ahead.T, behind.T
        ahead, behind = log_fading(ahead), log_fading(behind)
        cum_f = exact_dot(upto, ahead)
        cum_b = exact_dot(since, behind)
        reader[:, :size] = (query * jnp.exp(cum_f)).astype(BF16)
        reader[:, size:] = (query * jnp.exp(cum_b)).astype(BF16)
        sums = []
        for i in range(count):
            part = slice(i * BLK, (i + 1) * BLK)
            own_f, own_b = ahead[part], behind[part]
            local_f = exact_dot(upto[:BLK, :BLK], own_f)
            local_b = exact_dot(since[:BLK, :BLK], own_b)
            q_i, k_i = query[part], key[part]
            score_f = fast_dot(q_i * jnp.exp(local_f), k_i * jnp.exp(-local_f), on_last)
            score_b = fast_dot(q_i * jnp.exp(local_b), k_i * jnp.exp(-local_b), on_last)
            score = jnp.where(lower, score_f, 0.0) + jnp.where(upper, score_b, 0.0)
            sums.append(fast_dot(score, value[part]))
        for j in range(count):
            part = slice(j * BLK, (j + 1) * BLK)
            if j + 1 < count:
                rest = slice((j + 1) * BLK, length)
                end = cum_f[(j + 1) * BLK - 1 : (j + 1) * BLK]
                gone = fast_dot(
                    query[rest] * jnp.exp(cum_f[rest] - end),
                    key[part] * jnp.exp(end - cum_f[part]),
                    on_last,
                )
                carried = fast_dot(gone, value[part])
                for i in range(j + 1, count):
                    sums[i] = sums[i] + carried[(i - j - 1) * BLK : (i - j) * BLK]
            if j > 0:
                rest = slice(0, j * BLK)
                end = cum_b[j * BLK : j * BLK + 1]
                gone = fast_dot(
                    query[rest] * jnp.exp(cum_b[rest] - end),
                    key[part] * jnp.exp(end - cum_b[part]),
                    on_last,
                )
                carried = fast_dot(gone, value[part])
                for i in range(j):
                    sums[i] = sums[i] + carried[i * BLK : (i + 1) * BLK]
        for i in range(count):
            mixed[i * BLK : (i + 1) * BLK, at : at + 128] = sums[i]
        at += 128


def heads_kernel(
    core, local, reader_one, reader_two, carried, opened, own, sent, both, spread
):
    width = 128
    length = local.shape[0]
    spread[...] = carried[...].astype(F32)
    peers = spread.shape[0] // 16

    def state(first, last):
        return jnp.concatenate(
            [
                spread[pl.ds(kind * 6 + n, peers, stride=16), :]
                for kind in range(2)
                for n in range(first, last)
            ],
            axis=0,
        )

    at = 0
    for reader, held in ((reader_one, state(0, 2)), (reader_two, state(2, 6))):
        mixed = local[:, at : at + width] + fast_dot(reader[...], held)
        scale = lax.rsqrt(jnp.mean(mixed * mixed, axis=-1, keepdims=True) + 1e-06)
        heads = (mixed * scale * opened[:, at : at + width]).astype(BF16)
        for turn in range(length // STEP):
            where = (turn // 2) * STEP
            both[turn % 2, where : where + STEP, at : at + width] = heads[
                turn * STEP : (turn + 1) * STEP
            ]
        at += width
    own[...] = both[core[0]]
    sent[...] = both[1 - core[0]]


def routing_kernel(where, routes, affinity, chosen, weighted):
    core, first = where[0], where[1]
    rows = routes.shape[1]
    slots = chosen.shape[0]
    experts = slots // SLOTS
    half = rows // 2
    row, col = grid_of(rows)
    inner = lax.rem(row, half)
    turn = jnp.where(row < half, core, 1 - core)
    token = 2 * STEP * lax.div(inner, STEP) + STEP * turn + lax.rem(inner, STEP)
    order = (token == col).astype(F32)
    lane = lax.broadcasted_iota(jnp.int32, (experts, rows), 0)
    named = [routes[k : k + 1, :] for k in range(2)]
    hot = [(lane == name).astype(F32) for name in named]
    before = fast_dot(hot[0] + hot[1], (row < col).astype(BF16))
    share = affinity[...]
    share = share / jnp.sum(share, axis=0, keepdims=True)
    lines = []
    for k in range(2):
        rank = jnp.sum(hot[k] * before, axis=0, keepdims=True).astype(jnp.int32) - first
        inside = (rank >= 0) & (rank < SLOTS)
        spot = jnp.where(inside, rank * experts + named[k], -1)
        lines.append(spot.astype(F32))
    lines += [share[0:1, :], share[1:2, :]]
    lines = jnp.concatenate(lines + [jnp.zeros((4, rows), F32)], axis=0)
    flat = exact_dot(lines, order, ((1,), (1,)))
    tall = exact_dot(order, lines, ((1,), (1,)))
    place = lax.broadcasted_iota(jnp.int32, (slots, rows), 0).astype(F32)
    hit = (place == flat[0:1, :]) | (place == flat[1:2, :])
    chosen[...] = hit.astype(F32).astype(BF16)
    place = lax.broadcasted_iota(jnp.int32, (rows, slots), 1).astype(F32)
    scaled = jnp.where(place == tall[:, 0:1], tall[:, 2:3], 0.0)
    scaled = scaled + jnp.where(place == tall[:, 1:2], tall[:, 3:4], 0.0)
    weighted[...] = scaled.astype(BF16)


def loosen(packed, spread):
    for n in range(spread.shape[0]):
        spread[n] = packed[:, n * 128 : (n + 1) * 128].astype(F32)


def tighten(spread, packed):
    for n in range(spread.shape[0]):
        packed[:, n * 128 : (n + 1) * 128] = spread[n].astype(BF16)


def strided(first, peers):
    return pl.ds(first, peers, stride=LINES)


def taken(spread, part, each):
    peers = spread.shape[1] // LINES
    return jnp.concatenate(
        [
            jnp.concatenate(
                [spread[n, strided(part * each + slot, peers), :] for slot in range(each)],
                axis=0,
            ).astype(BF16)
            for n in range(spread.shape[0])
        ],
        axis=1,
    )


def placed(spread, part, each, value):
    peers = spread.shape[1] // LINES
    for n in range(value.shape[1] // 128):
        for slot in range(each):
            spread[n, strided(part * each + slot, peers), :] = value[
                slot * peers : (slot + 1) * peers, n * 128 : (n + 1) * 128
            ]


def dispatch_kernel(chosen, own, other, out, spread):
    wide = out.shape[1]
    each = SLOTS // SPLIT
    for part in range(LINES // each):
        lanes = slice(part * wide, (part + 1) * wide)
        both = jnp.concatenate([own[:, lanes], other[:, lanes]], axis=0)
        placed(spread, part, each, fast_dot(chosen[...], both))
    tighten(spread, out)


def expert_kernel(
    rows, own, near, side, far, out, spread, own_here, near_here, side_here, far_here, marks
):
    packs = (own_here, near_here, side_here, far_here)
    copies = fetched((own, near, side, far), packs, marks)
    wide = rows.shape[1]
    hidden = own.shape[1] // 2
    each = SLOTS // SPLIT
    parts = LINES // each
    loosen(rows, spread)
    x = jnp.concatenate([taken(spread, part, each) for part in range(parts)], axis=1)
    features = parts * wide
    acts = []
    for copy, pack in zip(copies, packs):
        copy.wait()
        both = fast_dot(x, pack[:features, :])
        gate, upward = both[:, :hidden], both[:, hidden:]
        acts.append((gate * jax.nn.sigmoid(gate) * upward).astype(BF16))
    acts = [jnp.concatenate(acts[:2], axis=1), jnp.concatenate(acts[2:], axis=1)]
    step = 2 * hidden
    found = []
    for n in range(features // step):
        here = slice(features + n * hidden, features + (n + 1) * hidden)
        value = 0.0
        for act, pair in zip(acts, (packs[:2], packs[2:])):
            value = value + fast_dot(act, jnp.concatenate([pack[here, :] for pack in pair], axis=0))
        found.append(value)
        if (n + 1) * step % wide == 0:
            placed(spread, n * step // wide, each, jnp.concatenate(found, axis=1))
            found = []
    tighten(spread, out)


def combine_kernel(weighted, *refs):
    returned, own, sent, spread = refs[:SPLIT], refs[SPLIT], refs[SPLIT + 1], refs[SPLIT + 2 :]
    half = own.shape[0]
    wide = returned[0].shape[1]
    each = SLOTS // SPLIT
    for packed, held in zip(returned, spread):
        loosen(packed, held)
    for part in range(LINES // each):
        lanes = slice(part * wide, (part + 1) * wide)
        rows = jnp.concatenate([taken(held, part, each) for held in spread], axis=0)
        value = fast_dot(weighted[...], rows)
        own[:, lanes] = value[:half]
        sent[:, lanes] = value[half:].astype(BF16)


def settle_kernel(parts, stream, gain, settled, copies):
    total = 0.0
    for place in range(parts.shape[0]):
        total = total + parts[place].astype(F32)
    attn = total.astype(BF16).astype(F32)
    found = layer_norm(stream[...].astype(F32) + attn, gain[...])
    settled[...] = found
    for place in range(parts.shape[0]):
        copies[place] = found.astype(BF16)


def finish_kernel(parts, settled, gain, out):
    total = 0.0
    for place in range(parts.shape[0]):
        total = total + parts[place].astype(F32)
    out[...] = layer_norm(settled[...] + total, gain[...]).astype(BF16)


def join_kernel(own, got, out):
    out[...] = (own[...] + got[...].astype(F32)).astype(BF16)


def project_kernel(own, got, proj, other, out, proj_here, marks):
    copies = fetched((proj,), (proj_here,), marks)
    theirs = fast_dot(got[...], other[...])
    copies[0].wait()
    width = out.shape[1]
    step = width // 4
    for n in range(4):
        lanes = slice(n * step, (n + 1) * step)
        value = theirs[:, lanes] + fast_dot(own[...], proj_here[:, lanes])
        out[:, lanes] = value.astype(BF16)


def layer_norm(values, gain):
    mean = jnp.mean(values, axis=-1, keepdims=True)
    spread = jnp.mean(jnp.square(values - mean), axis=-1, keepdims=True)
    return (values - mean) * lax.rsqrt(spread + 1e-05) * gain


def exchange(pieces, axis):
    return lax.all_to_all(pieces, axis, split_axis=0, concat_axis=0, tiled=True)


def swapped(value, axis):
    return lax.ppermute(value, axis, SWAP)


def tied(value, after):
    return lax.optimization_barrier((value, after))[0]


def body(
    query_one,
    key_one,
    value_one,
    gate_one,
    decay_one,
    query_two,
    key_two,
    value_two,
    gate_two,
    decay_two,
    head_gain,
    proj_one,
    proj_two,
    stream,
    gain_mix,
    gain_moe,
    routes,
    affinity,
    expert_gate,
    expert_up,
    expert_down,
):
    return layer(
        query_one.T,
        key_one.T,
        value_one,
        gate_one,
        jnp.swapaxes(decay_one, 1, 2),
        query_two,
        key_two,
        value_two,
        gate_two,
        decay_two,
        head_gain,
        proj_one,
        proj_two,
        stream,
        gain_mix,
        gain_moe,
        routes,
        affinity,
        expert_gate,
        expert_up,
        expert_down,
    )


def layer(
    query_one,
    key_one,
    value_one,
    gate_one,
    decay_one,
    query_two,
    key_two,
    value_two,
    gate_two,
    decay_two,
    head_gain,
    proj_one,
    proj_two,
    stream,
    gain_mix,
    gain_moe,
    routes,
    affinity,
    expert_gate,
    expert_up,
    expert_down,
):
    rows = query_two.shape[0]
    width = stream.shape[1]
    peers = lax.axis_size(SP)
    chips = lax.axis_size(Y)
    tp_count = lax.axis_size(TP)
    own_rows = rows // tp_count
    half = rows // 2
    core = lax.axis_index("c")
    tp_rank = lax.axis_index(TP)
    group = lax.axis_index(("b", "c"))
    hidden = expert_gate.shape[2]
    slots = peers * SLOTS
    each = slots // SPLIT
    wide = width * SLOTS // SPLIT // LINES
    keys = DK_A + DK_B
    shape = jax.ShapeDtypeStruct

    def scratch(items):
        held = [pltpu.VMEM(item.shape, item.dtype) for item in items]
        return held, pltpu.SemaphoreType.DMA((len(items),))

    early = (decay_one, decay_two, key_one, value_one, key_two, value_two)
    moves = (expert_gate, expert_up, expert_down, proj_one, proj_two, stream)
    held, marks = scratch(early)
    pieces_rows = 4 * keys
    blocks = width // (2 * hidden)
    pieces = call(
        states_kernel,
        pltpu.HBM((pieces_rows, 128), BF16),
        *early,
        far=range(len(early)),
        scratch=held + [pltpu.VMEM((pieces_rows, 128), F32), marks],
    )
    arrived = exchange(pieces.reshape(peers, pieces_rows // peers, 128), SP)
    pack, proj, stream_own = call(
        pack_kernel,
        [
            pltpu.HBM((width + blocks * hidden, 2 * hidden), BF16),
            pltpu.HBM((2 * hidden, width), BF16),
            shape((own_rows, width), BF16),
        ],
        tp_rank.reshape(1).astype(jnp.int32),
        *moves,
        far=range(1, 1 + len(moves)),
        scratch=[pltpu.SemaphoreType.DMA((5 + blocks,))],
    )
    near = swapped(pack, "b")
    side = swapped(pack, "c")
    proj_other = swapped(proj, "c")
    late = (
        query_one,
        key_one,
        value_one,
        decay_one,
        query_two,
        key_two,
        value_two,
        decay_two,
        gate_one,
        gate_two,
    )
    held, marks = scratch(late)
    local, reader_one, reader_two, opened = call(
        local_kernel,
        [
            shape((rows, 256), F32),
            shape((rows, 2 * DK_A), BF16),
            shape((rows, 2 * DK_B), BF16),
            shape((rows, 256), F32),
        ],
        *late,
        head_gain.reshape(1, 128),
        far=range(len(late)),
        scratch=held + [marks],
    )
    chosen, weighted = call(
        routing_kernel,
        [pltpu.HBM((slots, rows), BF16), pltpu.HBM((rows, slots), BF16)],
        jnp.stack([core, group * SLOTS]).astype(jnp.int32),
        routes.T,
        affinity.T,
    )
    starts = call(
        scan_kernel, pltpu.HBM((peers, 16, 128), BF16), arrived
    )
    carried = exchange(starts, SP).reshape(peers * 16, 128)
    heads_own, heads_sent = call(
        heads_kernel,
        [shape((half, 256), BF16)] * 2,
        core.reshape(1).astype(jnp.int32),
        local,
        reader_one,
        reader_two,
        carried,
        opened,
        scratch=[pltpu.VMEM((2, half, 256), BF16), pltpu.VMEM((peers * 16, 128), F32)],
    )
    far = swapped(tied(near, heads_own), "c")
    heads_got = swapped(heads_sent, "c")
    part = call(
        project_kernel,
        pltpu.HBM((half, width), BF16),
        heads_own,
        heads_got,
        proj,
        proj_other,
        far=(2,),
        scratch=[pltpu.VMEM((2 * hidden, width), BF16), pltpu.SemaphoreType.DMA((1,))],
    )
    attn = exchange(part.reshape(chips, own_rows, width), Y)
    settled, mine = call(
        settle_kernel,
        [pltpu.HBM((own_rows, width), F32), pltpu.HBM((chips, own_rows, width), BF16)],
        attn,
        stream_own,
        gain_mix.reshape(1, width),
    )
    moe_own = exchange(mine, Y).reshape(half, width)
    moe_other = swapped(moe_own, "c")
    lines = peers * LINES
    spread = [pltpu.VMEM((wide // 128, lines, 128), F32)]
    returned = []
    for turn in range(SPLIT):
        outgoing = call(
            dispatch_kernel,
            pltpu.HBM((lines, wide), BF16),
            chosen[turn * each : (turn + 1) * each],
            moe_own,
            moe_other,
            scratch=spread,
        )
        complete = exchange(outgoing.reshape(peers, LINES, wide), SP)
        partial = call(
            expert_kernel,
            pltpu.HBM((lines, wide), BF16),
            complete.reshape(lines, wide),
            pack,
            near,
            side,
            far,
            far=range(1, 5),
            scratch=spread
            + [pltpu.VMEM(pack.shape, BF16)] * 4
            + [pltpu.SemaphoreType.DMA((4,))],
        )
        arrived = exchange(partial.reshape(peers, LINES, wide), SP)
        returned.append(arrived.reshape(lines, wide))
    term_own, term_sent = call(
        combine_kernel,
        [shape((half, width), F32), shape((half, width), BF16)],
        weighted,
        *returned,
        scratch=spread * SPLIT,
    )
    term = call(join_kernel, pltpu.HBM((half, width), BF16), term_own, swapped(term_sent, "c"))
    mixture = exchange(term.reshape(chips, own_rows, width), Y)
    return call(
        finish_kernel,
        shape((own_rows, width), BF16),
        mixture,
        settled,
        gain_moe.reshape(1, width),
    )


def solution(mesh):
    finer = Mesh(mesh.devices.reshape(8, 4, 4, 2, 2), ALL)
    return jax.shard_map(
        body,
        mesh=finer,
        in_specs=(
            P(SP, TP),
            P(SP, TP),
            P(SP, TP),
            P(SP, TP),
            P(None, SP, TP),
            P(SP, TP),
            P(SP, TP),
            P(SP, TP),
            P(SP, TP),
            P(None, SP, TP),
            P(),
            P(TP, None),
            P(TP, None),
            P(SP, None),
            P(),
            P(),
            P(SP, None),
            P(SP, None),
            P(SP, None, TP),
            P(SP, None, TP),
            P(SP, TP, None),
        ),
        out_specs=P(ALL, None),
        check_vma=False,
    )
```

```python
import jax
import jax.numpy as jnp
from jax import lax
from jax.experimental import pallas as pl
from jax.experimental.pallas import tpu as pltpu
from jax.sharding import Mesh
from jax.sharding import PartitionSpec as P


DK_A = 64
DK_B = 128
BLK = 64
SHARERS = 4
SLOTS = 6
STEP = 16
SPLIT = 1
LINES = SHARERS * SLOTS
SP = ("z", "x")
Y = ("p", "b")
TP = ("p", "b", "c")
ALL = ("z", "x", "p", "b", "c")
SWAP = [(0, 1), (1, 0)]
F32 = jnp.float32
BF16 = jnp.bfloat16
VMEM_LIMIT = 32 * 1024 * 1024
normalizer_sharpness = 16.0


def call(kernel, outs, *args, far=(), scratch=()):
    single = not isinstance(outs, (list, tuple))
    shapes = [outs] if single else list(outs)
    vmem = pl.BlockSpec(memory_space=pltpu.VMEM)
    smem = pl.BlockSpec(memory_space=pltpu.SMEM)
    found = pl.pallas_call(
        kernel,
        out_shape=shapes,
        in_specs=[
            pl.BlockSpec(memory_space=pltpu.HBM)
            if k in far
            else smem
            if arg.ndim == 1
            else vmem
            for k, arg in enumerate(args)
        ],
        out_specs=[vmem] * len(shapes),
        scratch_shapes=list(scratch),
        compiler_params=pltpu.CompilerParams(vmem_limit_bytes=VMEM_LIMIT),
    )(
        *(
            pltpu.with_memory_space_constraint(arg, pltpu.HBM) if k in far else arg
            for k, arg in enumerate(args)
        )
    )
    return found[0] if single else found


def fetched(sources, places, marks):
    copies = [
        pltpu.make_async_copy(source, place, marks.at[k])
        for k, (source, place) in enumerate(zip(sources, places))
    ]
    for copy in copies:
        copy.start()
    return copies


def exact_dot(a, b, dims=((1,), (0,))):
    return lax.dot_general(
        a, b, (dims, ((), ())), precision=lax.Precision.HIGHEST, preferred_element_type=F32
    )


def fast_dot(a, b, dims=((1,), (0,))):
    return lax.dot_general(
        a.astype(BF16), b.astype(BF16), (dims, ((), ())), preferred_element_type=F32
    )


def thirds(value):
    high = value.astype(BF16)
    rest = value - high.astype(F32)
    middle = rest.astype(BF16)
    return high, middle, (rest - middle.astype(F32)).astype(BF16)


def sums_left(mask, value):
    high, middle, low = thirds(value)
    return fast_dot(mask, high) + (fast_dot(mask, middle) + fast_dot(mask, low))


def sums_right(value, mask, dims=((1,), (0,))):
    high, middle, low = thirds(value)
    return fast_dot(high, mask, dims) + (fast_dot(middle, mask, dims) + fast_dot(low, mask, dims))


def log_fading(pre):
    return (jnp.minimum(pre, 0.0) - jnp.log1p(jnp.exp(-jnp.abs(pre)))) / normalizer_sharpness


def grid_of(length):
    row = lax.broadcasted_iota(jnp.int32, (length, length), 0)
    col = lax.broadcasted_iota(jnp.int32, (length, length), 1)
    return row, col


def states_kernel(
    d1h, d2h, k1h, v1h, k2h, v2h, pieces, d1, d2, k1, v1, k2, v2, spread, marks
):
    copies = fetched((d1h, d2h, k1h, v1h, k2h, v2h), (d1, d2, k1, v1, k2, v2), marks)
    size, length = k1.shape
    peers = spread.shape[0] // 24
    row, col = grid_of(length)
    above = (row < col).astype(F32).astype(BF16)
    below = (row > col).astype(F32).astype(BF16)
    ones = jnp.ones((length, 128), BF16)

    def put(value, kind, first):
        for n in range(value.shape[0] // peers):
            spread[pl.ds(kind * 6 + first + n, peers, stride=24), :] = value[
                n * peers : (n + 1) * peers
            ]

    copies[0].wait()
    ahead, behind = log_fading(d1[0]), log_fading(d1[1])
    fade_f = jnp.exp(sums_right(ahead, below))
    fade_b = jnp.exp(sums_right(behind, above))
    put(sums_right(ahead, ones), 2, 0)
    put(sums_right(behind, ones), 3, 0)
    copies[1].wait()
    ahead, behind = log_fading(d2[0]), log_fading(d2[1])
    wide_f = jnp.exp(sums_left(above, ahead))
    wide_b = jnp.exp(sums_left(below, behind))
    across = ((0,), (0,))
    put(sums_right(ahead, ones, across), 2, size // peers)
    put(sums_right(behind, ones, across), 3, size // peers)
    copies[2].wait()
    copies[3].wait()
    key, value = k1[...].astype(F32), v1[...]
    put(fast_dot(key * fade_f, value), 0, 0)
    put(fast_dot(key * fade_b, value), 1, 0)
    copies[4].wait()
    copies[5].wait()
    key, value = k2[...].astype(F32), v2[...]
    put(fast_dot(key * wide_f, value, across), 0, size // peers)
    put(fast_dot(key * wide_b, value, across), 1, size // peers)
    pieces[...] = spread[...].astype(BF16)


def pack_kernel(gate, up, down, pack, moves):
    features, hidden = gate.shape[1:]
    sources = [gate.at[0], up.at[0]]
    places = [pack.at[:features, :hidden], pack.at[:features, hidden:]]
    for n in range(down.shape[2] // (2 * hidden)):
        sources.append(down.at[0, :, 2 * hidden * n : 2 * hidden * (n + 1)])
        places.append(pack.at[features + hidden * n : features + hidden * (n + 1), :])
    for copy in fetched(sources, places, moves):
        copy.wait()


def gather_kernel(where, one, two, stream, proj, own, moves):
    rows, hidden = own.shape[0], one.shape[0]
    mine = stream.at[pl.ds(pl.multiple_of(where[0] * rows, rows), rows), :]
    places = (proj.at[:hidden, :], proj.at[hidden:, :], own)
    for copy in fetched((one, two, mine), places, moves):
        copy.wait()


def scan_kernel(pieces, out):
    peers, rows2, lanes = pieces.shape
    rows = rows2 // 2
    half = rows // 2
    forward = lax.broadcasted_iota(jnp.int32, (rows, lanes), 0) < half
    state = jnp.zeros((rows, lanes), F32)
    found = []
    for place in range(peers):
        found.append(state)
        if place + 1 < peers:
            whole = pieces[place].astype(F32)
            state = jnp.exp(whole[rows:]) * state + whole[:rows]
    state = jnp.zeros((rows, lanes), F32)
    for place in reversed(range(peers)):
        out[place, :rows] = jnp.where(forward, found[place], state).astype(BF16)
        out[place, rows:] = jnp.zeros((out.shape[1] - rows, lanes), BF16)
        if place > 0:
            whole = pieces[place].astype(F32)
            state = jnp.exp(whole[rows:]) * state + whole[:rows]


def local_kernel(
    q1h, k1h, v1h, d1h, q2h, k2h, v2h, d2h, g1h, g2h, gain,
    mixed, reader_one, reader_two, opened,
    q1, k1, v1, d1, q2, k2, v2, d2, g1, g2, marks,
):
    copies = fetched(
        (q1h, k1h, v1h, d1h, q2h, k2h, v2h, d2h, g1h, g2h),
        (q1, k1, v1, d1, q2, k2, v2, d2, g1, g2),
        marks,
    )
    for copy in copies:
        copy.wait()
    length = v1.shape[0]
    for place, gate in enumerate((g1, g2)):
        value = gate[...].astype(F32)
        opened[:, place * 128 : (place + 1) * 128] = value * jax.nn.sigmoid(value) * gain[...]
    count = length // BLK
    row, col = grid_of(length)
    upto = (col <= row).astype(F32).astype(BF16)
    since = (col >= row).astype(F32).astype(BF16)
    brow, bcol = grid_of(BLK)
    lower, upper = bcol <= brow, bcol >= brow
    on_last = ((1,), (1,))
    at = 0
    for q_ref, k_ref, v_ref, d_ref, reader in (
        (q1, k1, v1, d1, reader_one),
        (q2, k2, v2, d2, reader_two),
    ):
        size = reader.shape[1] // 2
        query = q_ref[...].astype(F32) * size ** (-0.5)
        key = k_ref[...].astype(F32)
        value = v_ref[...]
        ahead, behind = d_ref[0], d_ref[1]
        if size == DK_A:
            query, key, ahead, behind = query.T, key.T, ahead.T, behind.T
        ahead, behind = log_fading(ahead), log_fading(behind)
        cum_f = sums_left(upto, ahead)
        cum_b = sums_left(since, behind)
        reader[:, :size] = (query * jnp.exp(cum_f)).astype(BF16)
        reader[:, size:] = (query * jnp.exp(cum_b)).astype(BF16)
        sums = []
        for i in range(count):
            part = slice(i * BLK, (i + 1) * BLK)
            local_f, local_b = cum_f[part], cum_b[part]
            if i > 0:
                local_f = local_f - cum_f[i * BLK - 1 : i * BLK]
            if i + 1 < count:
                local_b = local_b - cum_b[(i + 1) * BLK : (i + 1) * BLK + 1]
            q_i, k_i = query[part], key[part]
            score_f = fast_dot(q_i * jnp.exp(local_f), k_i * jnp.exp(-local_f), on_last)
            score_b = fast_dot(q_i * jnp.exp(local_b), k_i * jnp.exp(-local_b), on_last)
            score = jnp.where(lower, score_f, 0.0) + jnp.where(upper, score_b, 0.0)
            sums.append(fast_dot(score, value[part]))
        for j in range(count):
            part = slice(j * BLK, (j + 1) * BLK)
            if j + 1 < count:
                rest = slice((j + 1) * BLK, length)
                end = cum_f[(j + 1) * BLK - 1 : (j + 1) * BLK]
                gone = fast_dot(
                    query[rest] * jnp.exp(cum_f[rest] - end),
                    key[part] * jnp.exp(end - cum_f[part]),
                    on_last,
                )
                carried = fast_dot(gone, value[part])
                for i in range(j + 1, count):
                    sums[i] = sums[i] + carried[(i - j - 1) * BLK : (i - j) * BLK]
            if j > 0:
                rest = slice(0, j * BLK)
                end = cum_b[j * BLK : j * BLK + 1]
                gone = fast_dot(
                    query[rest] * jnp.exp(cum_b[rest] - end),
                    key[part] * jnp.exp(end - cum_b[part]),
                    on_last,
                )
                carried = fast_dot(gone, value[part])
                for i in range(j):
                    sums[i] = sums[i] + carried[i * BLK : (i + 1) * BLK]
        for i in range(count):
            mixed[i * BLK : (i + 1) * BLK, at : at + 128] = sums[i]
        at += 128


def heads_kernel(
    core, local, reader_one, reader_two, carried, opened, own, sent, both, spread
):
    width = 128
    length = local.shape[0]
    spread[...] = carried[...].astype(F32)
    peers = spread.shape[0] // 16

    def state(first, last):
        return jnp.concatenate(
            [
                spread[pl.ds(kind * 6 + n, peers, stride=16), :]
                for kind in range(2)
                for n in range(first, last)
            ],
            axis=0,
        )

    at = 0
    for reader, held in ((reader_one, state(0, 2)), (reader_two, state(2, 6))):
        mixed = local[:, at : at + width] + fast_dot(reader[...], held)
        scale = lax.rsqrt(jnp.mean(mixed * mixed, axis=-1, keepdims=True) + 1e-06)
        heads = (mixed * scale * opened[:, at : at + width]).astype(BF16)
        for turn in range(length // STEP):
            where = (turn // 2) * STEP
            both[turn % 2, where : where + STEP, at : at + width] = heads[
                turn * STEP : (turn + 1) * STEP
            ]
        at += width
    own[...] = both[core[0]]
    sent[...] = both[1 - core[0]]


def routing_kernel(where, routes, affinity, chosen, weighted):
    core, first = where[0], where[1]
    rows = routes.shape[1]
    slots = chosen.shape[0]
    experts = slots // SLOTS
    half = rows // 2
    row, col = grid_of(rows)
    inner = lax.rem(row, half)
    turn = jnp.where(row < half, core, 1 - core)
    token = 2 * STEP * lax.div(inner, STEP) + STEP * turn + lax.rem(inner, STEP)
    order = (token == col).astype(F32)
    lane = lax.broadcasted_iota(jnp.int32, (experts, rows), 0)
    named = [routes[k : k + 1, :] for k in range(2)]
    hot = [(lane == name).astype(F32) for name in named]
    before = fast_dot(hot[0] + hot[1], (row < col).astype(BF16))
    share = affinity[...]
    share = share / jnp.sum(share, axis=0, keepdims=True)
    lines = []
    for k in range(2):
        rank = jnp.sum(hot[k] * before, axis=0, keepdims=True).astype(jnp.int32) - first
        inside = (rank >= 0) & (rank < SLOTS)
        spot = jnp.where(inside, rank * experts + named[k], -1)
        lines.append(spot.astype(F32))
    lines += [share[0:1, :], share[1:2, :]]
    lines = jnp.concatenate(lines + [jnp.zeros((4, rows), F32)], axis=0)
    flat = exact_dot(lines, order, ((1,), (1,)))
    tall = exact_dot(order, lines, ((1,), (1,)))
    place = lax.broadcasted_iota(jnp.int32, (slots, rows), 0).astype(F32)
    hit = (place == flat[0:1, :]) | (place == flat[1:2, :])
    chosen[...] = hit.astype(F32).astype(BF16)
    place = lax.broadcasted_iota(jnp.int32, (rows, slots), 1).astype(F32)
    scaled = jnp.where(place == tall[:, 0:1], tall[:, 2:3], 0.0)
    scaled = scaled + jnp.where(place == tall[:, 1:2], tall[:, 3:4], 0.0)
    weighted[...] = scaled.astype(BF16)


def loosen(packed, spread):
    for n in range(spread.shape[0]):
        spread[n] = packed[:, n * 128 : (n + 1) * 128].astype(F32)


def tighten(spread, packed):
    for n in range(spread.shape[0]):
        packed[:, n * 128 : (n + 1) * 128] = spread[n].astype(BF16)


def strided(first, peers):
    return pl.ds(first, peers, stride=LINES)


def taken(spread, part, each):
    peers = spread.shape[1] // LINES
    return jnp.concatenate(
        [
            jnp.concatenate(
                [spread[n, strided(part * each + slot, peers), :] for slot in range(each)],
                axis=0,
            ).astype(BF16)
            for n in range(spread.shape[0])
        ],
        axis=1,
    )


def placed(spread, part, each, value):
    peers = spread.shape[1] // LINES
    for n in range(value.shape[1] // 128):
        for slot in range(each):
            spread[n, strided(part * each + slot, peers), :] = value[
                slot * peers : (slot + 1) * peers, n * 128 : (n + 1) * 128
            ]


def dispatch_kernel(chosen, own, other, side, far, out, side_here, far_here, spread, marks):
    copies = fetched((side, far), (side_here, far_here), marks)
    wide = out.shape[1]
    each = SLOTS // SPLIT
    for part in range(LINES // each):
        lanes = slice(part * wide, (part + 1) * wide)
        both = jnp.concatenate([own[:, lanes], other[:, lanes]], axis=0)
        placed(spread, part, each, fast_dot(chosen[...], both))
    tighten(spread, out)
    for copy in copies:
        copy.wait()


def expert_kernel(rows, own, near, side, far, out, spread):
    packs = (own, near, side, far)
    wide = rows.shape[1]
    hidden = own.shape[1] // 2
    each = SLOTS // SPLIT
    parts = LINES // each
    loosen(rows, spread)
    x = jnp.concatenate([taken(spread, part, each) for part in range(parts)], axis=1)
    features = parts * wide
    acts = []
    for pack in packs:
        both = fast_dot(x, pack[:features, :])
        gate, upward = both[:, :hidden], both[:, hidden:]
        acts.append((gate * jax.nn.sigmoid(gate) * upward).astype(BF16))
    acts = [jnp.concatenate(acts[:2], axis=1), jnp.concatenate(acts[2:], axis=1)]
    step = 2 * hidden
    found = []
    for n in range(features // step):
        here = slice(features + n * hidden, features + (n + 1) * hidden)
        value = 0.0
        for act, pair in zip(acts, (packs[:2], packs[2:])):
            value = value + fast_dot(act, jnp.concatenate([pack[here, :] for pack in pair], axis=0))
        found.append(value)
        if (n + 1) * step % wide == 0:
            placed(spread, n * step // wide, each, jnp.concatenate(found, axis=1))
            found = []
    tighten(spread, out)


def load_kernel(*refs):
    count = len(refs) // 2
    for copy in fetched(refs[:count], refs[count : 2 * count], refs[2 * count]):
        copy.wait()


def combine_kernel(weighted, *refs):
    returned, own, sent, spread = refs[:SPLIT], refs[SPLIT], refs[SPLIT + 1], refs[SPLIT + 2 :]
    half = own.shape[0]
    wide = returned[0].shape[1]
    each = SLOTS // SPLIT
    for packed, held in zip(returned, spread):
        loosen(packed, held)
    for part in range(LINES // each):
        lanes = slice(part * wide, (part + 1) * wide)
        rows = jnp.concatenate([taken(held, part, each) for held in spread], axis=0)
        value = fast_dot(weighted[...], rows)
        own[:, lanes] = value[:half]
        sent[:, lanes] = value[half:].astype(BF16)


def settle_kernel(parts, stream, gain, settled, copies):
    total = 0.0
    for place in range(parts.shape[0]):
        total = total + parts[place].astype(F32)
    attn = total.astype(BF16).astype(F32)
    found = layer_norm(stream[...].astype(F32) + attn, gain[...])
    settled[...] = found
    for place in range(parts.shape[0]):
        copies[place] = found.astype(BF16)


def finish_kernel(parts, settled, gain, out):
    total = 0.0
    for place in range(parts.shape[0]):
        total = total + parts[place].astype(F32)
    out[...] = layer_norm(settled[...] + total, gain[...]).astype(BF16)


def join_kernel(own, got, out):
    out[...] = (own[...] + got[...].astype(F32)).astype(BF16)


def project_kernel(own, got, proj, other, out):
    width = out.shape[1]
    step = width // 4
    for n in range(4):
        lanes = slice(n * step, (n + 1) * step)
        value = fast_dot(got[...], other[:, lanes]) + fast_dot(own[...], proj[:, lanes])
        out[:, lanes] = value.astype(BF16)


def layer_norm(values, gain):
    mean = jnp.mean(values, axis=-1, keepdims=True)
    spread = jnp.mean(jnp.square(values - mean), axis=-1, keepdims=True)
    return (values - mean) * lax.rsqrt(spread + 1e-05) * gain


def exchange(pieces, axis):
    return lax.all_to_all(pieces, axis, split_axis=0, concat_axis=0, tiled=True)


def swapped(value, axis):
    return lax.ppermute(value, axis, SWAP)


def tied(value, after):
    return lax.optimization_barrier((value, after))[0]


def body(
    query_one,
    key_one,
    value_one,
    gate_one,
    decay_one,
    query_two,
    key_two,
    value_two,
    gate_two,
    decay_two,
    head_gain,
    proj_one,
    proj_two,
    stream,
    gain_mix,
    gain_moe,
    routes,
    affinity,
    expert_gate,
    expert_up,
    expert_down,
):
    return layer(
        query_one.T,
        key_one.T,
        value_one,
        gate_one,
        jnp.swapaxes(decay_one, 1, 2),
        query_two,
        key_two,
        value_two,
        gate_two,
        decay_two,
        head_gain,
        proj_one,
        proj_two,
        stream,
        gain_mix,
        gain_moe,
        routes,
        affinity,
        expert_gate,
        expert_up,
        expert_down,
    )


def layer(
    query_one,
    key_one,
    value_one,
    gate_one,
    decay_one,
    query_two,
    key_two,
    value_two,
    gate_two,
    decay_two,
    head_gain,
    proj_one,
    proj_two,
    stream,
    gain_mix,
    gain_moe,
    routes,
    affinity,
    expert_gate,
    expert_up,
    expert_down,
):
    rows = query_two.shape[0]
    width = stream.shape[1]
    peers = lax.axis_size(SP)
    chips = lax.axis_size(Y)
    tp_count = lax.axis_size(TP)
    own_rows = rows // tp_count
    half = rows // 2
    core = lax.axis_index("c")
    tp_rank = lax.axis_index(TP)
    group = lax.axis_index(("b", "c"))
    hidden = expert_gate.shape[2]
    slots = peers * SLOTS
    each = slots // SPLIT
    wide = width * SLOTS // SPLIT // LINES
    keys = DK_A + DK_B
    shape = jax.ShapeDtypeStruct

    def scratch(items):
        held = [pltpu.VMEM(item.shape, item.dtype) for item in items]
        return held, pltpu.SemaphoreType.DMA((len(items),))

    early = (decay_one, decay_two, key_one, value_one, key_two, value_two)
    weights = (expert_gate, expert_up, expert_down)
    packed = (width + width // (2 * hidden) * hidden, 2 * hidden)
    held, marks = scratch(early)
    pieces_rows = 4 * keys
    blocks = width // (2 * hidden)
    pieces = call(
        states_kernel,
        pltpu.HBM((pieces_rows, 128), BF16),
        *early,
        far=range(len(early)),
        scratch=held + [pltpu.VMEM((pieces_rows, 128), F32), marks],
    )
    arrived = exchange(pieces.reshape(peers, pieces_rows // peers, 128), SP)
    pack = call(
        pack_kernel,
        pltpu.HBM(packed, BF16),
        *weights,
        far=range(len(weights)),
        scratch=[pltpu.SemaphoreType.DMA((2 + blocks,))],
    )
    proj, stream_own = call(
        gather_kernel,
        [pltpu.HBM((2 * hidden, width), BF16), shape((own_rows, width), BF16)],
        tp_rank.reshape(1).astype(jnp.int32),
        proj_one,
        proj_two,
        stream,
        far=(1, 2, 3),
        scratch=[pltpu.SemaphoreType.DMA((3,))],
    )
    near = swapped(pack, "b")
    side = swapped(pack, "c")
    proj_other = swapped(proj, "c")
    late = (
        query_one,
        key_one,
        value_one,
        decay_one,
        query_two,
        key_two,
        value_two,
        decay_two,
        gate_one,
        gate_two,
    )
    held, marks = scratch(late)
    local, reader_one, reader_two, opened = call(
        local_kernel,
        [
            shape((rows, 256), F32),
            shape((rows, 2 * DK_A), BF16),
            shape((rows, 2 * DK_B), BF16),
            shape((rows, 256), F32),
        ],
        *late,
        head_gain.reshape(1, 128),
        far=range(len(late)),
        scratch=held + [marks],
    )
    chosen, weighted = call(
        routing_kernel,
        [pltpu.HBM((slots, rows), BF16), pltpu.HBM((rows, slots), BF16)],
        jnp.stack([core, group * SLOTS]).astype(jnp.int32),
        routes.T,
        affinity.T,
    )
    starts = call(
        scan_kernel, pltpu.HBM((peers, 16, 128), BF16), arrived
    )
    carried = exchange(starts, SP).reshape(peers * 16, 128)
    heads_own, heads_sent = call(
        heads_kernel,
        [shape((half, 256), BF16)] * 2,
        core.reshape(1).astype(jnp.int32),
        local,
        reader_one,
        reader_two,
        carried,
        opened,
        scratch=[pltpu.VMEM((2, half, 256), BF16), pltpu.VMEM((peers * 16, 128), F32)],
    )
    far = swapped(tied(near, heads_own), "c")
    heads_got = swapped(heads_sent, "c")
    proj = call(
        load_kernel,
        shape((2 * hidden, width), BF16),
        proj,
        far=(0,),
        scratch=[pltpu.SemaphoreType.DMA((1,))],
    )
    part = call(
        project_kernel,
        pltpu.HBM((half, width), BF16),
        heads_own,
        heads_got,
        proj,
        proj_other,
    )
    attn = exchange(part.reshape(chips, own_rows, width), Y)
    settled, mine = call(
        settle_kernel,
        [pltpu.HBM((own_rows, width), F32), pltpu.HBM((chips, own_rows, width), BF16)],
        attn,
        stream_own,
        gain_mix.reshape(1, width),
    )
    moe_own = exchange(mine, Y).reshape(half, width)
    moe_other = swapped(moe_own, "c")
    lines = peers * LINES
    spread = [pltpu.VMEM((wide // 128, lines, 128), F32)]
    pack, near = call(
        load_kernel,
        [shape(packed, BF16)] * 2,
        pack,
        near,
        far=(0, 1),
        scratch=[pltpu.SemaphoreType.DMA((2,))],
    )
    returned = []
    for turn in range(SPLIT):
        outgoing, side, far = call(
            dispatch_kernel,
            [pltpu.HBM((lines, wide), BF16)] + [shape(packed, BF16)] * 2,
            chosen[turn * each : (turn + 1) * each],
            moe_own,
            moe_other,
            side,
            far,
            far=(3, 4),
            scratch=spread + [pltpu.SemaphoreType.DMA((2,))],
        )
        complete = exchange(outgoing.reshape(peers, LINES, wide), SP)
        partial = call(
            expert_kernel,
            pltpu.HBM((lines, wide), BF16),
            complete.reshape(lines, wide),
            pack,
            near,
            side,
            far,
            scratch=spread,
        )
        arrived = exchange(partial.reshape(peers, LINES, wide), SP)
        returned.append(arrived.reshape(lines, wide))
    term_own, term_sent = call(
        combine_kernel,
        [shape((half, width), F32), shape((half, width), BF16)],
        weighted,
        *returned,
        scratch=spread * SPLIT,
    )
    term = call(join_kernel, pltpu.HBM((half, width), BF16), term_own, swapped(term_sent, "c"))
    mixture = exchange(term.reshape(chips, own_rows, width), Y)
    return call(
        finish_kernel,
        shape((own_rows, width), BF16),
        mixture,
        settled,
        gain_moe.reshape(1, width),
    )


def solution(mesh):
    finer = Mesh(mesh.devices.reshape(8, 4, 4, 2, 2), ALL)
    return jax.shard_map(
        body,
        mesh=finer,
        in_specs=(
            P(SP, TP),
            P(SP, TP),
            P(SP, TP),
            P(SP, TP),
            P(None, SP, TP),
            P(SP, TP),
            P(SP, TP),
            P(SP, TP),
            P(SP, TP),
            P(None, SP, TP),
            P(),
            P(TP, None),
            P(TP, None),
            P(SP, None),
            P(),
            P(),
            P(SP, None),
            P(SP, None),
            P(SP, None, TP),
            P(SP, None, TP),
            P(SP, TP, None),
        ),
        out_specs=P(ALL, None),
        check_vma=False,
    )
```

```python
import jax
import jax.numpy as jnp
from jax import lax
from jax.experimental import pallas as pl
from jax.experimental.pallas import tpu as pltpu
from jax.sharding import Mesh
from jax.sharding import PartitionSpec as P


DK_A = 64
DK_B = 128
BLK = 64
SHARERS = 4
SLOTS = 6
STEP = 16
SPLIT = 1
LINES = SHARERS * SLOTS
SP = ("z", "x")
Y = ("p", "b")
TP = ("p", "b", "c")
ALL = ("z", "x", "p", "b", "c")
SWAP = [(0, 1), (1, 0)]
F32 = jnp.float32
BF16 = jnp.bfloat16
VMEM_LIMIT = 32 * 1024 * 1024
normalizer_sharpness = 16.0


def call(kernel, outs, *args, far=(), scratch=()):
    single = not isinstance(outs, (list, tuple))
    shapes = [outs] if single else list(outs)
    vmem = pl.BlockSpec(memory_space=pltpu.VMEM)
    smem = pl.BlockSpec(memory_space=pltpu.SMEM)
    found = pl.pallas_call(
        kernel,
        out_shape=shapes,
        in_specs=[
            pl.BlockSpec(memory_space=pltpu.HBM)
            if k in far
            else smem
            if arg.ndim == 1
            else vmem
            for k, arg in enumerate(args)
        ],
        out_specs=[vmem] * len(shapes),
        scratch_shapes=list(scratch),
        compiler_params=pltpu.CompilerParams(vmem_limit_bytes=VMEM_LIMIT),
    )(
        *(
            pltpu.with_memory_space_constraint(arg, pltpu.HBM) if k in far else arg
            for k, arg in enumerate(args)
        )
    )
    return found[0] if single else found


def fetched(sources, places, marks):
    copies = [
        pltpu.make_async_copy(source, place, marks.at[k])
        for k, (source, place) in enumerate(zip(sources, places))
    ]
    for copy in copies:
        copy.start()
    return copies


def exact_dot(a, b, dims=((1,), (0,))):
    return lax.dot_general(
        a, b, (dims, ((), ())), precision=lax.Precision.HIGHEST, preferred_element_type=F32
    )


def fast_dot(a, b, dims=((1,), (0,))):
    return lax.dot_general(
        a.astype(BF16), b.astype(BF16), (dims, ((), ())), preferred_element_type=F32
    )


def thirds(value):
    high = value.astype(BF16)
    rest = value - high.astype(F32)
    middle = rest.astype(BF16)
    return high, middle, (rest - middle.astype(F32)).astype(BF16)


def sums_left(mask, value):
    high, middle, low = thirds(value)
    return fast_dot(mask, high) + (fast_dot(mask, middle) + fast_dot(mask, low))


def sums_right(value, mask, dims=((1,), (0,))):
    high, middle, low = thirds(value)
    return fast_dot(high, mask, dims) + (fast_dot(middle, mask, dims) + fast_dot(low, mask, dims))


def log_fading(pre):
    return (jnp.minimum(pre, 0.0) - jnp.log1p(jnp.exp(-jnp.abs(pre)))) / normalizer_sharpness


def grid_of(length):
    row = lax.broadcasted_iota(jnp.int32, (length, length), 0)
    col = lax.broadcasted_iota(jnp.int32, (length, length), 1)
    return row, col


def states_kernel(
    d1h, d2h, k1h, v1h, k2h, v2h, pieces, d1, d2, k1, v1, k2, v2, spread, marks
):
    copies = fetched((d1h, d2h, k1h, v1h, k2h, v2h), (d1, d2, k1, v1, k2, v2), marks)
    size, length = k1.shape
    peers = spread.shape[0] // 24
    row, col = grid_of(length)
    above = (row < col).astype(F32).astype(BF16)
    below = (row > col).astype(F32).astype(BF16)
    ones = jnp.ones((length, 128), BF16)

    def put(value, kind, first):
        for n in range(value.shape[0] // peers):
            spread[pl.ds(kind * 6 + first + n, peers, stride=24), :] = value[
                n * peers : (n + 1) * peers
            ]

    copies[0].wait()
    ahead, behind = log_fading(d1[0]), log_fading(d1[1])
    fade_f = jnp.exp(sums_right(ahead, below))
    fade_b = jnp.exp(sums_right(behind, above))
    put(sums_right(ahead, ones), 2, 0)
    put(sums_right(behind, ones), 3, 0)
    copies[1].wait()
    ahead, behind = log_fading(d2[0]), log_fading(d2[1])
    wide_f = jnp.exp(sums_left(above, ahead))
    wide_b = jnp.exp(sums_left(below, behind))
    across = ((0,), (0,))
    put(sums_right(ahead, ones, across), 2, size // peers)
    put(sums_right(behind, ones, across), 3, size // peers)
    copies[2].wait()
    copies[3].wait()
    key, value = k1[...].astype(F32), v1[...]
    put(fast_dot(key * fade_f, value), 0, 0)
    put(fast_dot(key * fade_b, value), 1, 0)
    copies[4].wait()
    copies[5].wait()
    key, value = k2[...].astype(F32), v2[...]
    put(fast_dot(key * wide_f, value, across), 0, size // peers)
    put(fast_dot(key * wide_b, value, across), 1, size // peers)
    pieces[...] = spread[...].astype(BF16)


def pack_kernel(gate, up, down, pack, moves):
    features, hidden = gate.shape[1:]
    sources = [gate.at[0], up.at[0]]
    places = [pack.at[:features, :hidden], pack.at[:features, hidden:]]
    for n in range(down.shape[2] // (2 * hidden)):
        sources.append(down.at[0, :, 2 * hidden * n : 2 * hidden * (n + 1)])
        places.append(pack.at[features + hidden * n : features + hidden * (n + 1), :])
    for copy in fetched(sources, places, moves):
        copy.wait()


def gather_kernel(where, one, two, stream, proj, own, moves):
    rows, hidden = own.shape[0], one.shape[0]
    mine = stream.at[pl.ds(pl.multiple_of(where[0] * rows, rows), rows), :]
    places = (proj.at[:hidden, :], proj.at[hidden:, :], own)
    for copy in fetched((one, two, mine), places, moves):
        copy.wait()


def scan_kernel(pieces, out):
    peers, rows2, lanes = pieces.shape
    rows = rows2 // 2
    half = rows // 2
    forward = lax.broadcasted_iota(jnp.int32, (rows, lanes), 0) < half
    state = jnp.zeros((rows, lanes), F32)
    found = []
    for place in range(peers):
        found.append(state)
        if place + 1 < peers:
            whole = pieces[place].astype(F32)
            state = jnp.exp(whole[rows:]) * state + whole[:rows]
    state = jnp.zeros((rows, lanes), F32)
    for place in reversed(range(peers)):
        out[place, :rows] = jnp.where(forward, found[place], state).astype(BF16)
        out[place, rows:] = jnp.zeros((out.shape[1] - rows, lanes), BF16)
        if place > 0:
            whole = pieces[place].astype(F32)
            state = jnp.exp(whole[rows:]) * state + whole[:rows]


def local_kernel(
    q1h, k1h, v1h, d1h, q2h, k2h, v2h, d2h, g1h, g2h, gain,
    mixed, reader_one, reader_two, opened,
    q1, k1, v1, d1, q2, k2, v2, d2, g1, g2, marks,
):
    copies = fetched(
        (q1h, k1h, v1h, d1h, q2h, k2h, v2h, d2h, g1h, g2h),
        (q1, k1, v1, d1, q2, k2, v2, d2, g1, g2),
        marks,
    )
    for copy in copies:
        copy.wait()
    length = v1.shape[0]
    for place, gate in enumerate((g1, g2)):
        value = gate[...].astype(F32)
        opened[:, place * 128 : (place + 1) * 128] = value * jax.nn.sigmoid(value) * gain[...]
    count = length // BLK
    row, col = grid_of(length)
    upto = (col <= row).astype(F32).astype(BF16)
    since = (col >= row).astype(F32).astype(BF16)
    brow, bcol = grid_of(BLK)
    lower, upper = bcol <= brow, bcol >= brow
    on_last = ((1,), (1,))
    at = 0
    for q_ref, k_ref, v_ref, d_ref, reader in (
        (q1, k1, v1, d1, reader_one),
        (q2, k2, v2, d2, reader_two),
    ):
        size = reader.shape[1] // 2
        query = q_ref[...].astype(F32) * size ** (-0.5)
        key = k_ref[...].astype(F32)
        value = v_ref[...]
        ahead, behind = d_ref[0], d_ref[1]
        if size == DK_A:
            query, key, ahead, behind = query.T, key.T, ahead.T, behind.T
        ahead, behind = log_fading(ahead), log_fading(behind)
        cum_f = sums_left(upto, ahead)
        cum_b = sums_left(since, behind)
        reader[:, :size] = (query * jnp.exp(cum_f)).astype(BF16)
        reader[:, size:] = (query * jnp.exp(cum_b)).astype(BF16)
        sums = []
        for i in range(count):
            part = slice(i * BLK, (i + 1) * BLK)
            local_f, local_b = cum_f[part], cum_b[part]
            if i > 0:
                local_f = local_f - cum_f[i * BLK - 1 : i * BLK]
            if i + 1 < count:
                local_b = local_b - cum_b[(i + 1) * BLK : (i + 1) * BLK + 1]
            q_i, k_i = query[part], key[part]
            score_f = fast_dot(q_i * jnp.exp(local_f), k_i * jnp.exp(-local_f), on_last)
            score_b = fast_dot(q_i * jnp.exp(local_b), k_i * jnp.exp(-local_b), on_last)
            score = jnp.where(lower, score_f, 0.0) + jnp.where(upper, score_b, 0.0)
            sums.append(fast_dot(score, value[part]))
        for j in range(count):
            part = slice(j * BLK, (j + 1) * BLK)
            if j + 1 < count:
                rest = slice((j + 1) * BLK, length)
                end = cum_f[(j + 1) * BLK - 1 : (j + 1) * BLK]
                gone = fast_dot(
                    query[rest] * jnp.exp(cum_f[rest] - end),
                    key[part] * jnp.exp(end - cum_f[part]),
                    on_last,
                )
                carried = fast_dot(gone, value[part])
                for i in range(j + 1, count):
                    sums[i] = sums[i] + carried[(i - j - 1) * BLK : (i - j) * BLK]
            if j > 0:
                rest = slice(0, j * BLK)
                end = cum_b[j * BLK : j * BLK + 1]
                gone = fast_dot(
                    query[rest] * jnp.exp(cum_b[rest] - end),
                    key[part] * jnp.exp(end - cum_b[part]),
                    on_last,
                )
                carried = fast_dot(gone, value[part])
                for i in range(j):
                    sums[i] = sums[i] + carried[i * BLK : (i + 1) * BLK]
        for i in range(count):
            mixed[i * BLK : (i + 1) * BLK, at : at + 128] = sums[i]
        at += 128


def heads_kernel(
    core, local, reader_one, reader_two, carried, opened, own, sent, both, spread
):
    width = 128
    length = local.shape[0]
    spread[...] = carried[...].astype(F32)
    peers = spread.shape[0] // 16

    def state(first, last):
        return jnp.concatenate(
            [
                spread[pl.ds(kind * 6 + n, peers, stride=16), :]
                for kind in range(2)
                for n in range(first, last)
            ],
            axis=0,
        )

    at = 0
    for reader, held in ((reader_one, state(0, 2)), (reader_two, state(2, 6))):
        mixed = local[:, at : at + width] + fast_dot(reader[...], held)
        scale = lax.rsqrt(jnp.mean(mixed * mixed, axis=-1, keepdims=True) + 1e-06)
        heads = (mixed * scale * opened[:, at : at + width]).astype(BF16)
        for turn in range(length // STEP):
            where = (turn // 2) * STEP
            both[turn % 2, where : where + STEP, at : at + width] = heads[
                turn * STEP : (turn + 1) * STEP
            ]
        at += width
    own[...] = both[core[0]]
    sent[...] = both[1 - core[0]]


def routing_kernel(where, routes, affinity, chosen, weighted):
    core, first = where[0], where[1]
    rows = routes.shape[1]
    slots = chosen.shape[0]
    experts = slots // SLOTS
    half = rows // 2
    row, col = grid_of(rows)
    inner = lax.rem(row, half)
    turn = jnp.where(row < half, core, 1 - core)
    token = 2 * STEP * lax.div(inner, STEP) + STEP * turn + lax.rem(inner, STEP)
    order = (token == col).astype(F32)
    lane = lax.broadcasted_iota(jnp.int32, (experts, rows), 0)
    named = [routes[k : k + 1, :] for k in range(2)]
    hot = [(lane == name).astype(F32) for name in named]
    before = fast_dot(hot[0] + hot[1], (row < col).astype(BF16))
    share = affinity[...]
    share = share / jnp.sum(share, axis=0, keepdims=True)
    lines = []
    for k in range(2):
        rank = jnp.sum(hot[k] * before, axis=0, keepdims=True).astype(jnp.int32) - first
        inside = (rank >= 0) & (rank < SLOTS)
        spot = jnp.where(inside, rank * experts + named[k], -1)
        lines.append(spot.astype(F32))
    lines += [share[0:1, :], share[1:2, :]]
    lines = jnp.concatenate(lines + [jnp.zeros((4, rows), F32)], axis=0)
    flat = exact_dot(lines, order, ((1,), (1,)))
    tall = exact_dot(order, lines, ((1,), (1,)))
    place = lax.broadcasted_iota(jnp.int32, (slots, rows), 0).astype(F32)
    hit = (place == flat[0:1, :]) | (place == flat[1:2, :])
    chosen[...] = hit.astype(F32).astype(BF16)
    place = lax.broadcasted_iota(jnp.int32, (rows, slots), 1).astype(F32)
    scaled = jnp.where(place == tall[:, 0:1], tall[:, 2:3], 0.0)
    scaled = scaled + jnp.where(place == tall[:, 1:2], tall[:, 3:4], 0.0)
    weighted[...] = scaled.astype(BF16)


def loosen(packed, spread):
    for n in range(spread.shape[0]):
        spread[n] = packed[:, n * 128 : (n + 1) * 128].astype(F32)


def tighten(spread, packed):
    for n in range(spread.shape[0]):
        packed[:, n * 128 : (n + 1) * 128] = spread[n].astype(BF16)


def strided(first, peers):
    return pl.ds(first, peers, stride=LINES)


def taken(spread, part, each):
    peers = spread.shape[1] // LINES
    return jnp.concatenate(
        [
            jnp.concatenate(
                [spread[n, strided(part * each + slot, peers), :] for slot in range(each)],
                axis=0,
            ).astype(BF16)
            for n in range(spread.shape[0])
        ],
        axis=1,
    )


def placed(spread, part, each, value):
    peers = spread.shape[1] // LINES
    for n in range(value.shape[1] // 128):
        for slot in range(each):
            spread[n, strided(part * each + slot, peers), :] = value[
                slot * peers : (slot + 1) * peers, n * 128 : (n + 1) * 128
            ]


def dispatch_kernel(chosen, own, other, far, out, far_here, spread, marks):
    copies = fetched((far,), (far_here,), marks)
    wide = out.shape[1]
    each = SLOTS // SPLIT
    for part in range(LINES // each):
        lanes = slice(part * wide, (part + 1) * wide)
        both = jnp.concatenate([own[:, lanes], other[:, lanes]], axis=0)
        placed(spread, part, each, fast_dot(chosen[...], both))
    tighten(spread, out)
    for copy in copies:
        copy.wait()


def expert_kernel(rows, own, near, side, far, out, spread):
    packs = (own, near, side, far)
    wide = rows.shape[1]
    hidden = own.shape[1] // 2
    each = SLOTS // SPLIT
    parts = LINES // each
    loosen(rows, spread)
    x = jnp.concatenate([taken(spread, part, each) for part in range(parts)], axis=1)
    features = parts * wide
    acts = []
    for pack in packs:
        both = fast_dot(x, pack[:features, :])
        gate, upward = both[:, :hidden], both[:, hidden:]
        acts.append((gate * jax.nn.sigmoid(gate) * upward).astype(BF16))
    acts = [jnp.concatenate(acts[:2], axis=1), jnp.concatenate(acts[2:], axis=1)]
    step = 2 * hidden
    found = []
    for n in range(features // step):
        here = slice(features + n * hidden, features + (n + 1) * hidden)
        value = 0.0
        for act, pair in zip(acts, (packs[:2], packs[2:])):
            value = value + fast_dot(act, jnp.concatenate([pack[here, :] for pack in pair], axis=0))
        found.append(value)
        if (n + 1) * step % wide == 0:
            placed(spread, n * step // wide, each, jnp.concatenate(found, axis=1))
            found = []
    tighten(spread, out)


def load_kernel(*refs):
    count = len(refs) // 2
    for copy in fetched(refs[:count], refs[count : 2 * count], refs[2 * count]):
        copy.wait()


def combine_kernel(weighted, *refs):
    returned, own, sent, spread = refs[:SPLIT], refs[SPLIT], refs[SPLIT + 1], refs[SPLIT + 2 :]
    half = own.shape[0]
    wide = returned[0].shape[1]
    each = SLOTS // SPLIT
    for packed, held in zip(returned, spread):
        loosen(packed, held)
    for part in range(LINES // each):
        lanes = slice(part * wide, (part + 1) * wide)
        rows = jnp.concatenate([taken(held, part, each) for held in spread], axis=0)
        value = fast_dot(weighted[...], rows)
        own[:, lanes] = value[:half]
        sent[:, lanes] = value[half:].astype(BF16)


def settle_kernel(parts, stream, gain, settled, copies):
    total = 0.0
    for place in range(parts.shape[0]):
        total = total + parts[place].astype(F32)
    attn = total.astype(BF16).astype(F32)
    found = layer_norm(stream[...].astype(F32) + attn, gain[...])
    settled[...] = found
    for place in range(parts.shape[0]):
        copies[place] = found.astype(BF16)


def finish_kernel(parts, settled, gain, out):
    total = 0.0
    for place in range(parts.shape[0]):
        total = total + parts[place].astype(F32)
    out[...] = layer_norm(settled[...] + total, gain[...]).astype(BF16)


def join_kernel(own, got, out):
    out[...] = (own[...] + got[...].astype(F32)).astype(BF16)


def project_kernel(own, got, proj, other, out):
    width = out.shape[1]
    step = width // 4
    for n in range(4):
        lanes = slice(n * step, (n + 1) * step)
        value = fast_dot(got[...], other[:, lanes]) + fast_dot(own[...], proj[:, lanes])
        out[:, lanes] = value.astype(BF16)


def layer_norm(values, gain):
    mean = jnp.mean(values, axis=-1, keepdims=True)
    spread = jnp.mean(jnp.square(values - mean), axis=-1, keepdims=True)
    return (values - mean) * lax.rsqrt(spread + 1e-05) * gain


def exchange(pieces, axis):
    return lax.all_to_all(pieces, axis, split_axis=0, concat_axis=0, tiled=True)


def swapped(value, axis):
    return lax.ppermute(value, axis, SWAP)


def tied(value, after):
    return lax.optimization_barrier((value, after))[0]


def body(
    query_one,
    key_one,
    value_one,
    gate_one,
    decay_one,
    query_two,
    key_two,
    value_two,
    gate_two,
    decay_two,
    head_gain,
    proj_one,
    proj_two,
    stream,
    gain_mix,
    gain_moe,
    routes,
    affinity,
    expert_gate,
    expert_up,
    expert_down,
):
    return layer(
        query_one.T,
        key_one.T,
        value_one,
        gate_one,
        jnp.swapaxes(decay_one, 1, 2),
        query_two,
        key_two,
        value_two,
        gate_two,
        decay_two,
        head_gain,
        proj_one,
        proj_two,
        stream,
        gain_mix,
        gain_moe,
        routes,
        affinity,
        expert_gate,
        expert_up,
        expert_down,
    )


def layer(
    query_one,
    key_one,
    value_one,
    gate_one,
    decay_one,
    query_two,
    key_two,
    value_two,
    gate_two,
    decay_two,
    head_gain,
    proj_one,
    proj_two,
    stream,
    gain_mix,
    gain_moe,
    routes,
    affinity,
    expert_gate,
    expert_up,
    expert_down,
):
    rows = query_two.shape[0]
    width = stream.shape[1]
    peers = lax.axis_size(SP)
    chips = lax.axis_size(Y)
    tp_count = lax.axis_size(TP)
    own_rows = rows // tp_count
    half = rows // 2
    core = lax.axis_index("c")
    tp_rank = lax.axis_index(TP)
    group = lax.axis_index(("b", "c"))
    hidden = expert_gate.shape[2]
    slots = peers * SLOTS
    each = slots // SPLIT
    wide = width * SLOTS // SPLIT // LINES
    keys = DK_A + DK_B
    shape = jax.ShapeDtypeStruct

    def scratch(items):
        held = [pltpu.VMEM(item.shape, item.dtype) for item in items]
        return held, pltpu.SemaphoreType.DMA((len(items),))

    early = (decay_one, decay_two, key_one, value_one, key_two, value_two)
    weights = (expert_gate, expert_up, expert_down)
    packed = (width + width // (2 * hidden) * hidden, 2 * hidden)
    held, marks = scratch(early)
    pieces_rows = 4 * keys
    blocks = width // (2 * hidden)
    pieces = call(
        states_kernel,
        pltpu.HBM((pieces_rows, 128), BF16),
        *early,
        far=range(len(early)),
        scratch=held + [pltpu.VMEM((pieces_rows, 128), F32), marks],
    )
    arrived = exchange(pieces.reshape(peers, pieces_rows // peers, 128), SP)
    pack = call(
        pack_kernel,
        shape(packed, BF16),
        *weights,
        far=range(len(weights)),
        scratch=[pltpu.SemaphoreType.DMA((2 + blocks,))],
    )
    proj, stream_own = call(
        gather_kernel,
        [pltpu.HBM((2 * hidden, width), BF16), shape((own_rows, width), BF16)],
        tp_rank.reshape(1).astype(jnp.int32),
        proj_one,
        proj_two,
        stream,
        far=(1, 2, 3),
        scratch=[pltpu.SemaphoreType.DMA((3,))],
    )
    near = swapped(pack, "b")
    side = swapped(pack, "c")
    proj_other = swapped(proj, "c")
    late = (
        query_one,
        key_one,
        value_one,
        decay_one,
        query_two,
        key_two,
        value_two,
        decay_two,
        gate_one,
        gate_two,
    )
    held, marks = scratch(late)
    local, reader_one, reader_two, opened = call(
        local_kernel,
        [
            shape((rows, 256), F32),
            shape((rows, 2 * DK_A), BF16),
            shape((rows, 2 * DK_B), BF16),
            shape((rows, 256), F32),
        ],
        *late,
        head_gain.reshape(1, 128),
        far=range(len(late)),
        scratch=held + [marks],
    )
    chosen, weighted = call(
        routing_kernel,
        [pltpu.HBM((slots, rows), BF16), pltpu.HBM((rows, slots), BF16)],
        jnp.stack([core, group * SLOTS]).astype(jnp.int32),
        routes.T,
        affinity.T,
    )
    starts = call(
        scan_kernel, pltpu.HBM((peers, 16, 128), BF16), arrived
    )
    carried = exchange(starts, SP).reshape(peers * 16, 128)
    heads_own, heads_sent = call(
        heads_kernel,
        [shape((half, 256), BF16)] * 2,
        core.reshape(1).astype(jnp.int32),
        local,
        reader_one,
        reader_two,
        carried,
        opened,
        scratch=[pltpu.VMEM((2, half, 256), BF16), pltpu.VMEM((peers * 16, 128), F32)],
    )
    far = swapped(tied(near, heads_own), "c")
    heads_got = swapped(heads_sent, "c")
    proj = call(
        load_kernel,
        shape((2 * hidden, width), BF16),
        proj,
        far=(0,),
        scratch=[pltpu.SemaphoreType.DMA((1,))],
    )
    part = call(
        project_kernel,
        pltpu.HBM((half, width), BF16),
        heads_own,
        heads_got,
        proj,
        proj_other,
    )
    attn = exchange(part.reshape(chips, own_rows, width), Y)
    settled, mine = call(
        settle_kernel,
        [pltpu.HBM((own_rows, width), F32), pltpu.HBM((chips, own_rows, width), BF16)],
        attn,
        stream_own,
        gain_mix.reshape(1, width),
    )
    moe_own = exchange(mine, Y).reshape(half, width)
    moe_other = swapped(moe_own, "c")
    lines = peers * LINES
    spread = [pltpu.VMEM((wide // 128, lines, 128), F32)]
    near, side = call(
        load_kernel,
        [shape(packed, BF16)] * 2,
        near,
        side,
        far=(0, 1),
        scratch=[pltpu.SemaphoreType.DMA((2,))],
    )
    returned = []
    for turn in range(SPLIT):
        outgoing, far = call(
            dispatch_kernel,
            [pltpu.HBM((lines, wide), BF16), shape(packed, BF16)],
            chosen[turn * each : (turn + 1) * each],
            moe_own,
            moe_other,
            far,
            far=(3,),
            scratch=spread + [pltpu.SemaphoreType.DMA((1,))],
        )
        complete = exchange(outgoing.reshape(peers, LINES, wide), SP)
        partial = call(
            expert_kernel,
            pltpu.HBM((lines, wide), BF16),
            complete.reshape(lines, wide),
            pack,
            near,
            side,
            far,
            scratch=spread,
        )
        arrived = exchange(partial.reshape(peers, LINES, wide), SP)
        returned.append(arrived.reshape(lines, wide))
    term_own, term_sent = call(
        combine_kernel,
        [shape((half, width), F32), shape((half, width), BF16)],
        weighted,
        *returned,
        scratch=spread * SPLIT,
    )
    term = call(join_kernel, pltpu.HBM((half, width), BF16), term_own, swapped(term_sent, "c"))
    mixture = exchange(term.reshape(chips, own_rows, width), Y)
    return call(
        finish_kernel,
        shape((own_rows, width), BF16),
        mixture,
        settled,
        gain_moe.reshape(1, width),
    )


def solution(mesh):
    finer = Mesh(mesh.devices.reshape(8, 4, 4, 2, 2), ALL)
    return jax.shard_map(
        body,
        mesh=finer,
        in_specs=(
            P(SP, TP),
            P(SP, TP),
            P(SP, TP),
            P(SP, TP),
            P(None, SP, TP),
            P(SP, TP),
            P(SP, TP),
            P(SP, TP),
            P(SP, TP),
            P(None, SP, TP),
            P(),
            P(TP, None),
            P(TP, None),
            P(SP, None),
            P(),
            P(),
            P(SP, None),
            P(SP, None),
            P(SP, None, TP),
            P(SP, None, TP),
            P(SP, TP, None),
        ),
        out_specs=P(ALL, None),
        check_vma=False,
    )
```
